128 devices in a mesh: sp: 16 (over z, y), tp: 8 (over x, core).
Axes of the slice: x: 4, y: 4, z: 4, core: 2. Of those that a mesh axis runs over, the one named last changes fastest.
Arguments:
- layer_input: bfloat16 [16, 4096, 2048], P(None, ('sp', 'tp')), may hold values from -6 to 6
- input_gain: float32 [2048], replicated, may hold values from 0.5 to 1.5
- narrowing_matrix: bfloat16 [2048, 512], replicated, may hold values from -0.125 to 0.125
- rotary_down: bfloat16 [2048, 64], replicated, may hold values from -0.125 to 0.125
- summary_scaling: float32 [512], replicated, may hold values from 0.5 to 1.5
- lookup_widening: bfloat16 [512, 16, 128], P('tp'), may hold values from -0.25 to 0.25
- payload_widening: bfloat16 [512, 16, 128], P('tp'), may hold values from -0.25 to 0.25
- query_nope: bfloat16 [16, 16, 128], P('sp', 'tp'), may hold values from -6 to 6
- query_rotary: bfloat16 [16, 16, 64], P('sp', 'tp'), may hold values from -6 to 6
Outputs:
- stored_summaries: bfloat16 [16, 4096, 512], P('sp', None, 'tp')
- rotary_cache: bfloat16 [16, 4096, 64], P('sp', None, 'tp')
- first_read: bfloat16 [16, 16, 128], P('sp', 'tp')
The draws below stay inside these ranges and needn't reach their ends.
All inputs are finite; a program needn't handle non-finite values.
Results may differ from the reference program's by a relative error of at most 0.02.
Values may be sent and summed in bfloat16 or wider, within the bound.
A program may use at most 64 MiB of HBM per device.

```python
import jax
import jax.numpy as jnp
from jax import lax

BREADTH = 2048
SQUEEZED_SPAN = 512
QK_ROPE = 64
PLAIN_MATCH_SPAN = 128
PAYLOAD_SPAN = 128
READERS = 16
BATCH_ITEMS = 16
SLOTS = 4096


def block_scale(stream_key, dims, shards, least, largest):
    def one(axis_at, blocks):
        heights = jax.random.uniform(jax.random.fold_in(jax.random.fold_in(stream_key, 6), axis_at), (blocks,), jnp.float32, least / len(shards), largest / len(shards))
        return jnp.repeat(jnp.exp(heights), dims[axis_at] // blocks).reshape((-1,) + (1,) * (len(dims) - axis_at - 1))

    factor_of = one(*shards[0])
    for cut in shards[1:]:
        factor_of = factor_of * one(*cut)
    return factor_of


def normal_values(stream_key, extent, deviation, reach, shards=(), held_as=jnp.bfloat16):
    level = block_scale(stream_key, extent, shards, -0.22, 0.18) if shards else 1.0
    entries = jax.random.normal(stream_key, extent, jnp.float32) * deviation * level
    return jnp.minimum(jnp.maximum(entries, -reach), reach).astype(held_as)


def setup_inputs(seed: int = 0) -> dict:
    keys = jax.random.split(jax.random.key(seed), 10)
    layer_input = normal_values(keys[0], (BATCH_ITEMS, SLOTS, BREADTH), 1.0, 6.0, ((1, 128),))
    input_gain = jnp.clip(1.0 + 0.1 * jax.random.normal(keys[1], (BREADTH,), jnp.float32), 0.5, 1.5)
    narrowing_matrix = normal_values(keys[2], (BREADTH, SQUEEZED_SPAN), BREADTH ** -0.5, 0.125)
    rotary_down = normal_values(keys[3], (BREADTH, QK_ROPE), BREADTH ** -0.5, 0.125)
    summary_scaling = jnp.clip(1.0 + 0.1 * jax.random.normal(keys[4], (SQUEEZED_SPAN,), jnp.float32), 0.5, 1.5)
    lookup_widening = normal_values(keys[5], (SQUEEZED_SPAN, READERS, PLAIN_MATCH_SPAN), SQUEEZED_SPAN ** -0.5, 0.25, ((0, 8),))
    payload_widening = normal_values(keys[6], (SQUEEZED_SPAN, READERS, PAYLOAD_SPAN), SQUEEZED_SPAN ** -0.5, 0.25, ((0, 8),))
    query_nope = normal_values(keys[7], (BATCH_ITEMS, READERS, PLAIN_MATCH_SPAN), 1.0, 6.0, ((0, 16), (1, 8)))
    query_rotary = normal_values(keys[8], (BATCH_ITEMS, READERS, QK_ROPE), 1.0, 6.0, ((0, 16), (1, 8)))
    return {"layer_input": layer_input, "input_gain": input_gain, "narrowing_matrix": narrowing_matrix, "rotary_down": rotary_down, "summary_scaling": summary_scaling, "lookup_widening": lookup_widening, "payload_widening": payload_widening, "query_nope": query_nope, "query_rotary": query_rotary}


norm_eps = 1e-06
rotary_base = 10000.0

def rescaled_lines(vector):
    return vector * lax.rsqrt(lax.optimization_barrier(jnp.mean(vector * vector, axis=-1, keepdims=True)) + norm_eps)

def rotate(vector, position):
    half_width = vector.shape[-1] // 2
    frequency = 1.0 / rotary_base ** (jnp.arange(half_width, dtype=jnp.float32) * 2.0 / vector.shape[-1])
    angles = position * frequency
    first_half = vector[..., :half_width]
    second_half = vector[..., half_width:]
    return jnp.concatenate([first_half * jnp.cos(angles) - second_half * jnp.sin(angles), second_half * jnp.cos(angles) + first_half * jnp.sin(angles)], axis=-1)

def reference(layer_input, input_gain, narrowing_matrix, rotary_down, summary_scaling, lookup_widening, payload_widening, query_nope, query_rotary):
    normed = (rescaled_lines(layer_input.astype(jnp.float32)) * input_gain).astype(jnp.bfloat16)
    flat_rows = normed.reshape(BATCH_ITEMS * SLOTS, BREADTH)
    hidden_summary = jnp.dot(flat_rows, narrowing_matrix, preferred_element_type=jnp.float32).astype(jnp.bfloat16)
    rotary = jnp.dot(flat_rows, rotary_down, preferred_element_type=jnp.float32).astype(jnp.bfloat16)
    stored_summaries = (rescaled_lines(hidden_summary.astype(jnp.float32)) * summary_scaling).astype(jnp.bfloat16).reshape(BATCH_ITEMS, SLOTS, SQUEEZED_SPAN)
    positions = jnp.arange(SLOTS, dtype=jnp.float32)[None, :, None]
    rotary_cache = rotate(rotary.astype(jnp.float32).reshape(BATCH_ITEMS, SLOTS, QK_ROPE), positions).astype(jnp.bfloat16)
    absorbed = jnp.einsum('shd,chd->shc', query_nope.astype(jnp.float32), lookup_widening.astype(jnp.float32)).astype(jnp.bfloat16)
    query_turned = rotate(query_rotary.astype(jnp.float32), jnp.float32(SLOTS)).astype(jnp.bfloat16)
    score_scale = (PLAIN_MATCH_SPAN + QK_ROPE) ** (-0.5)
    scores = (jnp.einsum('shc,spc->shp', absorbed.astype(jnp.float32), stored_summaries.astype(jnp.float32)) + jnp.einsum('shr,spr->shp', query_turned.astype(jnp.float32), rotary_cache.astype(jnp.float32))) * score_scale
    attention = jax.nn.softmax(scores, axis=-1).astype(jnp.bfloat16)
    context = jnp.einsum('shp,spc->shc', attention.astype(jnp.float32), stored_summaries.astype(jnp.float32)).astype(jnp.bfloat16)
    values = jnp.einsum('shc,chv->shv', context.astype(jnp.float32), payload_widening.astype(jnp.float32))
    first_read = rescaled_lines(values).astype(jnp.bfloat16)
    return (stored_summaries, rotary_cache, first_read)
```

```python
import jax
import jax.numpy as jnp
import numpy as np
from jax import lax
from jax.experimental import pallas as pl
from jax.experimental.pallas import tpu as pltpu
from jax.sharding import PartitionSpec as P

MESH = pl.DeviceIdType.MESH
EPS = 1e-6
ROPE_BASE = 10000.0
F32 = jnp.float32
BF16 = jnp.bfloat16

NT = (((1,), (1,)), ((), ()))


def trig_tables(blocks, rows, rope):
    half = rope // 2
    freq = 1.0 / ROPE_BASE ** (np.arange(half, dtype=np.float64) * 2.0 / rope)
    freq = np.concatenate([freq, freq])
    first = np.arange(blocks + 8, dtype=np.float64)[:, None] * rows * freq
    offset = np.arange(rows, dtype=np.float64)[:, None] * freq

    def both(angle):
        return np.concatenate([np.cos(angle), np.sin(angle)], axis=1).astype(np.float32)

    return both(first), both(offset)


def half_swap(v):
    half = v.shape[-1] // 2
    return jnp.concatenate([v[:, half:], v[:, :half]], axis=1)


def iota(shape, dim):
    return lax.broadcasted_iota(jnp.int32, shape, dim)


def kernel(
    x_hbm, gain_hbm, w_hbm, rd_hbm, scal_hbm, look_hbm, pay_hbm, qn_hbm, qr_hbm, tab_hbm, off_hbm,
    out_s, out_r, out_f,
    xb, gain, w, rd, scal, look, pay, tab, off,
    kst, kall, qn, qr, aall, pst, pall, ktst, rtst, krecv, rrecv, asc, arecv, sbuf,
    ostage, rstage, fstage,
    lsem, wsem, ksend, krsem, qsend, qrsem, asend, arsem, psend, prsem, k2send, k2rsem, csend, crsem, osem,
):
    sp, tp = lax.axis_index("sp"), lax.axis_index("tp")
    z, y = sp // 4, lax.rem(sp, 4)

    def sp_of(dz, dy):
        return lax.rem(z + dz, 4) * 4 + lax.rem(y + dy, 4)

    def tp_of(step):
        return lax.rem(tp + step, 8)

    def x_copy(n):
        return pltpu.make_async_copy(x_hbm.at[sp_of((n // 4 + 1) % 4, n % 4)], xb.at[n], lsem.at[n])

    loads = [
        pltpu.make_async_copy(src, dst, wsem.at[n])
        for n, (src, dst) in enumerate(
            (
                (gain_hbm, gain), (w_hbm, w), (rd_hbm, rd), (scal_hbm, scal), (tab_hbm, tab), (off_hbm, off),
                (look_hbm, look), (pay_hbm, pay), (qn_hbm, qn.at[tp]), (qr_hbm, qr.at[tp]),
            )
        )
    ]
    for n in range(4):
        x_copy(n).start()
    for c in loads[:6]:
        c.start()
    for n in range(4, 16):
        x_copy(n).start()
    for c in loads[6:]:
        c.start()

    barrier = pltpu.get_barrier_semaphore()

    def greet_sp(n, _):
        pl.semaphore_signal(barrier, inc=1, device_id=(lax.rem(sp + n, 16), tp), device_id_type=MESH)
        return 0

    def greet_tp(n, _):
        pl.semaphore_signal(barrier, inc=1, device_id=(sp, tp_of(n)), device_id_type=MESH)
        return 0

    lax.fori_loop(1, 16, greet_sp, 0)
    lax.fori_loop(1, 8, greet_tp, 0)

    def to_tp(src, dst, send, recv, step):
        return pltpu.make_async_remote_copy(
            src_ref=src, dst_ref=dst, send_sem=send, recv_sem=recv,
            device_id=(sp, tp_of(step)), device_id_type=MESH,
        )

    def q_copies(step, at):
        return (
            to_tp(qn_hbm, qn.at[at], qsend.at[0, step], qrsem.at[0, at], step),
            to_tp(qr_hbm, qr.at[at], qsend.at[1, step], qrsem.at[1, at], step),
        )

    def k_copy(n, dz, dy, slot):
        return pltpu.make_async_remote_copy(
            src_ref=kst.at[n], dst_ref=kall.at[slot], send_sem=ksend.at[n], recv_sem=krsem.at[slot],
            device_id=(sp_of(dz, dy), tp), device_id_type=MESH,
        )

    my_slot = 4 * z + lax.rem(y + tp, 4)

    for c in loads[:6]:
        c.wait()
    sign = jnp.where(iota((32, 64), 1) < 32, -1.0, 1.0).astype(F32)
    base = tab[pl.ds(sp * 8 + tp, 1), :]
    offs = off[...]
    cos = base[:, :64] * offs[:, :64] - base[:, 64:] * offs[:, 64:]
    sin = (base[:, 64:] * offs[:, :64] + base[:, :64] * offs[:, 64:]) * sign
    cos4 = jnp.concatenate([cos] * 4, axis=0)
    sin4 = jnp.concatenate([sin] * 4, axis=0)

    def project(k, _):
        dz = lax.rem(k + 1, 4)
        for dy in range(4):
            pltpu.make_async_copy(x_hbm.at[0], xb.at[4 * k + dy], lsem.at[4 * k + dy]).wait()
        xv = xb[pl.ds(4 * k, 4)].reshape(128, 2048).astype(F32)
        scale = lax.rsqrt(jnp.mean(xv * xv, axis=1, keepdims=True) + EPS)
        normed = (xv * scale * gain[...]).astype(BF16)
        latent = jnp.dot(normed, w[...], preferred_element_type=F32).astype(BF16).astype(F32)
        rot = lax.dot_general(normed, rd[...], NT, preferred_element_type=F32).astype(BF16).astype(F32)
        scale = lax.rsqrt(jnp.mean(latent * latent, axis=1, keepdims=True) + EPS)
        stored = (latent * scale * scal[...]).astype(BF16)
        turned = rot * cos4 + half_swap(rot) * sin4
        turned = jnp.concatenate([turned, jnp.zeros_like(turned)], axis=1).astype(BF16)
        kst[pl.ds(4 * k, 4), :, :512] = stored.reshape(4, 32, 512)
        kst[pl.ds(4 * k, 4), :, 512:] = turned.reshape(4, 32, 128)

        @pl.when(k == 3)
        def _():
            kall[my_slot, :, :512] = stored[:32]
            kall[my_slot, :, 512:] = turned[:32]

        @pl.when(k == 0)
        def _():
            pl.semaphore_wait(barrier, 22)

            def send_q(step, _):
                for c in q_copies(step, tp):
                    c.start()
                return 0

            lax.fori_loop(1, 8, send_q, 0)

        for dy in range(1, 4):
            k_copy(4 * k + dy, dz, dy, my_slot).start()

        @pl.when(k < 3)
        def _():
            k_copy(4 * k, dz, 0, my_slot).start()

        return 0

    lax.fori_loop(0, 4, project, 0)

    for c in loads[6:]:
        c.wait()

    def wait_q(step, _):
        for c in q_copies(step, tp_of(8 - step)):
            c.wait_recv()
        return 0

    lax.fori_loop(1, 8, wait_q, 0)
    q_all = qn[...].astype(F32).reshape(16, 128).astype(BF16)
    t_all = qr[...].astype(F32).reshape(16, 64)
    parts = lax.dot_general(q_all, look[...], NT, preferred_element_type=F32)
    same = jnp.bitwise_and(iota((16, 1024), 1), 15) == iota((16, 1024), 0)
    parts = jnp.where(same, parts, 0.0).astype(BF16)
    pick = jnp.right_shift(iota((1024, 128), 0), 4) + 64 * lax.rem(tp, 2) == iota((1024, 128), 1)
    pick = jnp.where(pick, 1.0, 0.0).astype(BF16)
    aall[tp] = jnp.dot(parts, pick, preferred_element_type=F32).astype(BF16)
    last = tab[128:129, :]
    q_turn = t_all * last[:, :64] + half_swap(t_all) * (last[:, 64:] * sign[:1])
    q_turn = jnp.concatenate([q_turn, jnp.zeros_like(q_turn)], axis=1).astype(BF16)

    def a_copy(step, at):
        return to_tp(aall.at[tp], aall.at[at], asend.at[step], arsem.at[at], step)

    def send_a(step, _):
        a_copy(step, tp).start()
        return 0

    lax.fori_loop(1, 8, send_a, 0)

    row, col = iota((256, 256), 0), iota((256, 256), 1)
    wanted = jnp.bitwise_and(row, 15) * 16 + jnp.right_shift(row, 4)
    order = jnp.where(col == wanted, 1.0, 0.0).astype(BF16)
    for g in range(4):
        rows = jnp.dot(order, pay[256 * g : 256 * (g + 1), :], preferred_element_type=F32)
        pst[:, :, 16 * g : 16 * (g + 1), :] = rows.astype(BF16).reshape(8, 2, 16, 128)
    pall[:, pl.ds(pl.multiple_of(tp * 64, 64), 64), :] = pst[tp]

    def p_copy(step, at):
        there = pall.at[:, pl.ds(pl.multiple_of(at * 64, 64), 64), :]
        return to_tp(pst.at[tp_of(step)], there, psend.at[step], prsem.at[at], step)

    def send_p(step, _):
        p_copy(step, tp).start()
        return 0

    lax.fori_loop(1, 8, send_p, 0)

    def wait_a(step, _):
        a_copy(step, tp_of(8 - step)).wait_recv()
        return 0

    lax.fori_loop(1, 8, wait_a, 0)
    absorbed = jnp.concatenate([aall[2 * u] + aall[2 * u + 1] for u in range(4)] + [q_turn], axis=1)

    def k2_copies(step, g, at):
        return (
            to_tp(ktst.at[g, tp_of(step)], krecv.at[g, at], k2send.at[0, g, step], k2rsem.at[0, g, at], step),
            to_tp(rtst.at[g, tp_of(step)], rrecv.at[g, at], k2send.at[1, g, step], k2rsem.at[1, g, at], step),
        )

    def group_of(k):
        return lax.rem(z + 3 - k, 4)

    def spread(k, _):
        g = group_of(k)
        for dy in range(1, 4):
            k_copy(4 * k + dy, 0, dy, 4 * g + lax.rem(y + 4 - dy + tp, 4)).wait_recv()

        @pl.when(k < 3)
        def _():
            k_copy(4 * k, 0, 1, 4 * g + lax.rem(y + tp, 4)).wait_recv()

        turned_over = kall[pl.ds(4 * g, 4)].reshape(128, 640).T
        ktst[g] = turned_over[:512].reshape(8, 64, 128)
        rtst[g] = turned_over[512:576].astype(F32).reshape(8, 8, 128).astype(BF16)

        def send(step, _):
            for c in k2_copies(step, g, tp):
                c.start()
            return 0

        lax.fori_loop(1, 8, send, 0)
        krecv[g, tp] = ktst[g, tp]
        rrecv[g, tp] = rtst[g, tp]
        sbuf[k] = jnp.dot(absorbed, turned_over, preferred_element_type=F32) * (192.0 ** -0.5)
        return 0

    lax.fori_loop(0, 4, spread, 0)

    scores = jnp.concatenate([sbuf[k] for k in range(4)], axis=1)
    top = jnp.max(scores, axis=1, keepdims=True)
    weight = jnp.exp(scores - top)
    total = jnp.sum(weight, axis=1, keepdims=True)
    context = jnp.zeros((16, 512), F32)
    for k in range(4):
        rows = kall[pl.ds(4 * group_of(k), 4), :, :512].reshape(128, 512)
        context += jnp.dot(
            weight[:, 128 * k : 128 * (k + 1)].astype(BF16), rows, preferred_element_type=F32
        )
    stats = jnp.where(iota((16, 128), 1) < 64, top, total)
    for t in range(8):
        asc[t, :, :512] = context[2 * t : 2 * t + 2]
        asc[t, :, 512:] = stats[2 * t : 2 * t + 2]

    def c_copy(step, at):
        return to_tp(asc.at[tp_of(step)], arecv.at[at], csend.at[step], crsem.at[at], step)

    def send_c(step, _):
        c_copy(step, tp).start()
        return 0

    lax.fori_loop(1, 8, send_c, 0)
    arecv[tp] = asc[tp]

    def wait_c(step, _):
        c_copy(step, tp_of(8 - step)).wait_recv()
        p_copy(step, tp_of(8 - step)).wait_recv()
        return 0

    lax.fori_loop(1, 8, wait_c, 0)
    got = arecv[...]
    tops, totals = got[:, :, 512:513], got[:, :, 576:577]
    share = jnp.exp(tops - jnp.max(tops, axis=0, keepdims=True))
    summed = jnp.sum(got[:, :, :512] * share, axis=0) / jnp.sum(totals * share, axis=0)
    mixed = jnp.concatenate([summed, jnp.zeros((14, 512), F32)], axis=0).astype(BF16)
    first = jnp.dot(mixed, pall[0], preferred_element_type=F32)
    second = jnp.dot(mixed, pall[1], preferred_element_type=F32)
    values = jnp.where(iota((16, 128), 0) == 0, first, second)[:2]
    values = values * lax.rsqrt(jnp.mean(values * values, axis=1, keepdims=True) + EPS)
    fstage[...] = values.astype(BF16)
    pltpu.make_async_copy(fstage, out_f, osem.at[8]).start()

    def out_copies(g):
        lanes = pl.ds(pl.multiple_of(g * 1024, 1024), 1024)
        return (
            pltpu.make_async_copy(ostage.at[g], out_s.at[:, lanes], osem.at[g]),
            pltpu.make_async_copy(rstage.at[g], out_r.at[:, lanes], osem.at[4 + g]),
        )

    def finish(k, _):
        g = group_of(k)

        def wait(step, _):
            for c in k2_copies(step, g, tp_of(8 - step)):
                c.wait_recv()
            return 0

        lax.fori_loop(1, 8, wait, 0)
        for source, stage, rows in ((krecv, ostage, 64), (rrecv, rstage, 8)):
            lane = jnp.right_shift(iota((rows, 128), 1), 5)
            for u in range(2):
                blocks = [source[g, 4 * u + j].astype(F32) for j in range(4)]
                for a in range(4):
                    mine = [jnp.bitwise_and(lane - a, 3) == j for j in range(3)]
                    v = jnp.where(
                        mine[0], blocks[0], jnp.where(mine[1], blocks[1], jnp.where(mine[2], blocks[2], blocks[3]))
                    )
                    if a:
                        v = pltpu.roll(v, 128 - 32 * a, 1)
                    at = 256 * a + 128 * u
                    stage[g, :, at : at + 128] = v.astype(BF16)
        for c in out_copies(g):
            c.start()
        return 0

    lax.fori_loop(0, 4, finish, 0)

    def drain(step, _):
        for c in q_copies(step, tp) + (a_copy(step, tp), p_copy(step, tp), c_copy(step, tp)):
            c.wait_send()
        for g in range(4):
            for c in k2_copies(step, g, tp):
                c.wait_send()
        return 0

    lax.fori_loop(1, 8, drain, 0)
    for n in range(16):
        if n != 12:
            k_copy(n, (n // 4 + 1) % 4, n % 4, my_slot).wait_send()
    for g in range(4):
        for c in out_copies(g):
            c.wait()
    pltpu.make_async_copy(fstage, out_f, osem.at[8]).wait()


def solution(mesh):
    first, offset = trig_tables(128, 32, 64)

    def step(x, gain, w, rd, scal, look, payload, qn, qr):
        any_space = pl.BlockSpec(memory_space=pl.ANY)
        dma = pltpu.SemaphoreType.DMA
        stored, rotary, read = pl.pallas_call(
            kernel,
            out_shape=(
                jax.ShapeDtypeStruct((64, 4096), BF16),
                jax.ShapeDtypeStruct((8, 4096), BF16),
                jax.ShapeDtypeStruct((2, 128), BF16),
            ),
            in_specs=[any_space] * 11,
            out_specs=(any_space,) * 3,
            scratch_shapes=[
                pltpu.VMEM((16, 32, 2048), BF16),
                pltpu.VMEM((1, 2048), F32),
                pltpu.VMEM((2048, 512), BF16),
                pltpu.VMEM((64, 2048), BF16),
                pltpu.VMEM((1, 512), F32),
                pltpu.VMEM((1024, 128), BF16),
                pltpu.VMEM((1024, 128), BF16),
                pltpu.VMEM((136, 128), F32),
                pltpu.VMEM((32, 128), F32),
                pltpu.VMEM((16, 32, 640), BF16),
                pltpu.VMEM((16, 32, 640), BF16),
                pltpu.VMEM((8, 2, 128), BF16),
                pltpu.VMEM((8, 2, 64), BF16),
                pltpu.VMEM((8, 16, 128), BF16),
                pltpu.VMEM((8, 2, 64, 128), BF16),
                pltpu.VMEM((2, 512, 128), BF16),
                pltpu.VMEM((4, 8, 64, 128), BF16),
                pltpu.VMEM((4, 8, 8, 128), BF16),
                pltpu.VMEM((4, 8, 64, 128), BF16),
                pltpu.VMEM((4, 8, 8, 128), BF16),
                pltpu.VMEM((8, 2, 640), F32),
                pltpu.VMEM((8, 2, 640), F32),
                pltpu.VMEM((4, 16, 128), F32),
                pltpu.VMEM((4, 64, 1024), BF16),
                pltpu.VMEM((4, 8, 1024), BF16),
                pltpu.VMEM((2, 128), BF16),
                dma((16,)),
                dma((10,)),
                dma((16,)),
                dma((16,)),
                dma((2, 8)),
                dma((2, 8)),
                dma((8,)),
                dma((8,)),
                dma((8,)),
                dma((8,)),
                dma((2, 4, 8)),
                dma((2, 4, 8)),
                dma((8,)),
                dma((8,)),
                dma((9,)),
            ],
            compiler_params=pltpu.CompilerParams(
                collective_id=0, has_side_effects=True, vmem_limit_bytes=48 * 1024 * 1024
            ),
        )(
            x, gain.reshape(1, 2048), w, rd.T, scal.reshape(1, 512), look.reshape(1024, 128),
            payload.reshape(1024, 128), qn.reshape(2, 128), qr.reshape(2, 64), jnp.asarray(first), jnp.asarray(offset),
        )
        return stored.T[None], rotary.T[None], read[None]

    tp = "tp"
    both = ("sp", "tp")
    in_specs = (
        P(None, both, None), P(), P(), P(), P(), P(tp, None, None), P(tp, None, None),
        P("sp", tp, None), P("sp", tp, None),
    )
    out_specs = (P("sp", None, tp), P("sp", None, tp), P("sp", tp, None))
    return jax.shard_map(step, mesh=mesh, in_specs=in_specs, out_specs=out_specs, check_vma=False)
```

```python
import jax
import jax.numpy as jnp
import numpy as np
from jax import lax
from jax.experimental import pallas as pl
from jax.experimental.pallas import tpu as pltpu
from jax.sharding import PartitionSpec as P

MESH = pl.DeviceIdType.MESH
EPS = 1e-6
ROPE_BASE = 10000.0
F32 = jnp.float32
BF16 = jnp.bfloat16

NT = (((1,), (1,)), ((), ()))


def trig_tables(blocks, rows, rope):
    half = rope // 2
    freq = 1.0 / ROPE_BASE ** (np.arange(half, dtype=np.float64) * 2.0 / rope)
    freq = np.concatenate([freq, freq])
    first = np.arange(blocks + 8, dtype=np.float64)[:, None] * rows * freq
    offset = np.arange(rows, dtype=np.float64)[:, None] * freq

    def both(angle):
        return np.concatenate([np.cos(angle), np.sin(angle)], axis=1).astype(np.float32)

    return both(first), both(offset)


def half_swap(v):
    half = v.shape[-1] // 2
    return jnp.concatenate([v[:, half:], v[:, :half]], axis=1)


def iota(shape, dim):
    return lax.broadcasted_iota(jnp.int32, shape, dim)


def kernel(
    x_hbm, gain_hbm, w_hbm, rd_hbm, scal_hbm, look_hbm, pay_hbm, qn_hbm, qr_hbm, tab_hbm, off_hbm,
    krecv, rrecv, read_out,
    xb, gain, w, rd, scal, look, pay, tab, off,
    kst, kall, qn, qr, aall, pst, pall, ktst, rtst, asc, arecv, sbuf,
    lsem, wsem, ksend, krsem, qsend, qrsem, asend, arsem, psend, prsem, k2send, k2rsem, csend, crsem,
):
    sp, tp = lax.axis_index("sp"), lax.axis_index("tp")
    z, y = sp // 4, lax.rem(sp, 4)

    def sp_of(dz, dy):
        return lax.rem(z + dz, 4) * 4 + lax.rem(y + dy, 4)

    def tp_of(step):
        return lax.rem(tp + step, 8)

    def x_copy(n):
        return pltpu.make_async_copy(x_hbm.at[sp_of((n // 4 + 1) % 4, n % 4)], xb.at[n], lsem.at[n])

    loads = [
        pltpu.make_async_copy(src, dst, wsem.at[n])
        for n, (src, dst) in enumerate(
            (
                (gain_hbm, gain), (w_hbm, w), (rd_hbm, rd), (scal_hbm, scal), (tab_hbm, tab), (off_hbm, off),
                (look_hbm, look), (pay_hbm, pay), (qn_hbm, qn.at[tp]), (qr_hbm, qr.at[tp]),
            )
        )
    ]
    for n in range(4):
        x_copy(n).start()
    for c in loads[:6]:
        c.start()
    for n in range(4, 16):
        x_copy(n).start()
    for c in loads[6:]:
        c.start()

    barrier = pltpu.get_barrier_semaphore()

    def greet_sp(n, _):
        pl.semaphore_signal(barrier, inc=1, device_id=(lax.rem(sp + n, 16), tp), device_id_type=MESH)
        return 0

    def greet_tp(n, _):
        pl.semaphore_signal(barrier, inc=1, device_id=(sp, tp_of(n)), device_id_type=MESH)
        return 0

    lax.fori_loop(1, 16, greet_sp, 0)
    lax.fori_loop(1, 8, greet_tp, 0)

    def to_tp(src, dst, send, recv, step):
        return pltpu.make_async_remote_copy(
            src_ref=src, dst_ref=dst, send_sem=send, recv_sem=recv,
            device_id=(sp, tp_of(step)), device_id_type=MESH,
        )

    def q_copies(step, at):
        return (
            to_tp(qn_hbm, qn.at[at], qsend.at[0, step], qrsem.at[0, at], step),
            to_tp(qr_hbm, qr.at[at], qsend.at[1, step], qrsem.at[1, at], step),
        )

    def k_copy(n, dz, dy, slot):
        return pltpu.make_async_remote_copy(
            src_ref=kst.at[n], dst_ref=kall.at[slot], send_sem=ksend.at[n], recv_sem=krsem.at[slot],
            device_id=(sp_of(dz, dy), tp), device_id_type=MESH,
        )

    my_slot = 4 * z + lax.rem(y + tp, 4)

    for c in loads[:6]:
        c.wait()
    sign = jnp.where(iota((32, 64), 1) < 32, -1.0, 1.0).astype(F32)
    base = tab[pl.ds(sp * 8 + tp, 1), :]
    offs = off[...]
    cos = base[:, :64] * offs[:, :64] - base[:, 64:] * offs[:, 64:]
    sin = (base[:, 64:] * offs[:, :64] + base[:, :64] * offs[:, 64:]) * sign
    cos4 = jnp.concatenate([cos] * 4, axis=0)
    sin4 = jnp.concatenate([sin] * 4, axis=0)

    def project(k, _):
        dz = lax.rem(k + 1, 4)
        for dy in range(4):
            pltpu.make_async_copy(x_hbm.at[0], xb.at[4 * k + dy], lsem.at[4 * k + dy]).wait()
        xv = xb[pl.ds(4 * k, 4)].reshape(128, 2048).astype(F32)
        scale = lax.rsqrt(jnp.mean(xv * xv, axis=1, keepdims=True) + EPS)
        normed = (xv * scale * gain[...]).astype(BF16)
        latent = jnp.dot(normed, w[...], preferred_element_type=F32).astype(BF16).astype(F32)
        rot = lax.dot_general(normed, rd[...], NT, preferred_element_type=F32).astype(BF16).astype(F32)
        scale = lax.rsqrt(jnp.mean(latent * latent, axis=1, keepdims=True) + EPS)
        stored = (latent * scale * scal[...]).astype(BF16)
        turned = rot * cos4 + half_swap(rot) * sin4
        turned = jnp.concatenate([turned, jnp.zeros_like(turned)], axis=1).astype(BF16)
        kst[pl.ds(4 * k, 4), :, :512] = stored.reshape(4, 32, 512)
        kst[pl.ds(4 * k, 4), :, 512:] = turned.reshape(4, 32, 128)

        @pl.when(k == 3)
        def _():
            kall[my_slot, :, :512] = stored[:32]
            kall[my_slot, :, 512:] = turned[:32]

        @pl.when(k == 0)
        def _():
            pl.semaphore_wait(barrier, 22)

            def send_q(step, _):
                for c in q_copies(step, tp):
                    c.start()
                return 0

            lax.fori_loop(1, 8, send_q, 0)

        for dy in range(1, 4):
            k_copy(4 * k + dy, dz, dy, my_slot).start()

        @pl.when(k < 3)
        def _():
            k_copy(4 * k, dz, 0, my_slot).start()

        return 0

    lax.fori_loop(0, 4, project, 0)

    for c in loads[6:]:
        c.wait()

    def wait_q(step, _):
        for c in q_copies(step, tp_of(8 - step)):
            c.wait_recv()
        return 0

    lax.fori_loop(1, 8, wait_q, 0)
    q_all = qn[...].astype(F32).reshape(16, 128).astype(BF16)
    t_all = qr[...].astype(F32).reshape(16, 64)
    parts = lax.dot_general(q_all, look[...], NT, preferred_element_type=F32)
    same = jnp.bitwise_and(iota((16, 1024), 1), 15) == iota((16, 1024), 0)
    parts = jnp.where(same, parts, 0.0).astype(BF16)
    pick = jnp.right_shift(iota((1024, 128), 0), 4) + 64 * lax.rem(tp, 2) == iota((1024, 128), 1)
    pick = jnp.where(pick, 1.0, 0.0).astype(BF16)
    aall[tp] = jnp.dot(parts, pick, preferred_element_type=F32).astype(BF16)
    last = tab[128:129, :]
    q_turn = t_all * last[:, :64] + half_swap(t_all) * (last[:, 64:] * sign[:1])
    q_turn = jnp.concatenate([q_turn, jnp.zeros_like(q_turn)], axis=1).astype(BF16)

    def a_copy(step, at):
        return to_tp(aall.at[tp], aall.at[at], asend.at[step], arsem.at[at], step)

    def send_a(step, _):
        a_copy(step, tp).start()
        return 0

    lax.fori_loop(1, 8, send_a, 0)

    row, col = iota((256, 256), 0), iota((256, 256), 1)
    wanted = jnp.bitwise_and(row, 15) * 16 + jnp.right_shift(row, 4)
    order = jnp.where(col == wanted, 1.0, 0.0).astype(BF16)
    for g in range(4):
        rows = jnp.dot(order, pay[256 * g : 256 * (g + 1), :], preferred_element_type=F32)
        pst[:, :, 16 * g : 16 * (g + 1), :] = rows.astype(BF16).reshape(8, 2, 16, 128)
    pall[:, pl.ds(pl.multiple_of(tp * 64, 64), 64), :] = pst[tp]

    def p_copy(step, at):
        there = pall.at[:, pl.ds(pl.multiple_of(at * 64, 64), 64), :]
        return to_tp(pst.at[tp_of(step)], there, psend.at[step], prsem.at[at], step)

    def send_p(step, _):
        p_copy(step, tp).start()
        return 0

    lax.fori_loop(1, 8, send_p, 0)

    def wait_a(step, _):
        a_copy(step, tp_of(8 - step)).wait_recv()
        return 0

    lax.fori_loop(1, 8, wait_a, 0)
    absorbed = jnp.concatenate([aall[2 * u] + aall[2 * u + 1] for u in range(4)] + [q_turn], axis=1)

    def k2_copies(step, g, at):
        return (
            to_tp(ktst.at[g, tp_of(step)], krecv.at[g, at], k2send.at[0, g, step], k2rsem.at[0, g, at], step),
            to_tp(rtst.at[g, tp_of(step)], rrecv.at[g, at], k2send.at[1, g, step], k2rsem.at[1, g, at], step),
        )

    def group_of(k):
        return lax.rem(z + 3 - k, 4)

    def spread(k, _):
        g = group_of(k)
        for dy in range(1, 4):
            k_copy(4 * k + dy, 0, dy, 4 * g + lax.rem(y + 4 - dy + tp, 4)).wait_recv()

        @pl.when(k < 3)
        def _():
            k_copy(4 * k, 0, 1, 4 * g + lax.rem(y + tp, 4)).wait_recv()

        turned_over = kall[pl.ds(4 * g, 4)].reshape(128, 640).T
        ktst[g] = turned_over[:512].reshape(8, 64, 128)
        rtst[g] = turned_over[512:576].astype(F32).reshape(8, 8, 128).astype(BF16)

        def send(step, _):
            for c in k2_copies(step, g, tp):
                c.start()
            return 0

        lax.fori_loop(1, 8, send, 0)
        krecv[g, tp] = ktst[g, tp]
        rrecv[g, tp] = rtst[g, tp]
        sbuf[k] = jnp.dot(absorbed, turned_over, preferred_element_type=F32) * (192.0 ** -0.5)
        return 0

    lax.fori_loop(0, 4, spread, 0)

    scores = jnp.concatenate([sbuf[k] for k in range(4)], axis=1)
    top = jnp.max(scores, axis=1, keepdims=True)
    weight = jnp.exp(scores - top)
    total = jnp.sum(weight, axis=1, keepdims=True)
    context = jnp.zeros((16, 512), F32)
    for k in range(4):
        rows = kall[pl.ds(4 * group_of(k), 4), :, :512].reshape(128, 512)
        context += jnp.dot(
            weight[:, 128 * k : 128 * (k + 1)].astype(BF16), rows, preferred_element_type=F32
        )
    stats = jnp.where(iota((16, 128), 1) < 64, top, total)
    for t in range(8):
        asc[t, :, :512] = context[2 * t : 2 * t + 2]
        asc[t, :, 512:] = stats[2 * t : 2 * t + 2]

    def c_copy(step, at):
        return to_tp(asc.at[tp_of(step)], arecv.at[at], csend.at[step], crsem.at[at], step)

    def send_c(step, _):
        c_copy(step, tp).start()
        return 0

    lax.fori_loop(1, 8, send_c, 0)
    arecv[tp] = asc[tp]

    def wait_c(step, _):
        c_copy(step, tp_of(8 - step)).wait_recv()
        p_copy(step, tp_of(8 - step)).wait_recv()
        return 0

    lax.fori_loop(1, 8, wait_c, 0)
    got = arecv[...]
    tops, totals = got[:, :, 512:513], got[:, :, 576:577]
    share = jnp.exp(tops - jnp.max(tops, axis=0, keepdims=True))
    summed = jnp.sum(got[:, :, :512] * share, axis=0) / jnp.sum(totals * share, axis=0)
    mixed = jnp.concatenate([summed, jnp.zeros((14, 512), F32)], axis=0).astype(BF16)
    first = jnp.dot(mixed, pall[0], preferred_element_type=F32)
    second = jnp.dot(mixed, pall[1], preferred_element_type=F32)
    values = jnp.where(iota((16, 128), 0) == 0, first, second)[:2]
    values = values * lax.rsqrt(jnp.mean(values * values, axis=1, keepdims=True) + EPS)
    read_out[...] = values.astype(BF16)

    def wait_k2(step, _):
        for g in range(4):
            for c in k2_copies(step, g, tp_of(8 - step)):
                c.wait_recv()
        return 0

    lax.fori_loop(1, 8, wait_k2, 0)

    def drain(step, _):
        for c in q_copies(step, tp) + (a_copy(step, tp), p_copy(step, tp), c_copy(step, tp)):
            c.wait_send()
        for g in range(4):
            for c in k2_copies(step, g, tp):
                c.wait_send()
        return 0

    lax.fori_loop(1, 8, drain, 0)
    for n in range(16):
        if n != 12:
            k_copy(n, (n // 4 + 1) % 4, n % 4, my_slot).wait_send()


def arrange(krecv, rrecv, read_in, out_s, out_r, out_f, ostage, rstage, sem):
    read = pltpu.make_async_copy(read_in, out_f, sem.at[8])
    read.start()
    copies = [read]
    for g in range(4):
        for source, stage, rows in ((krecv, ostage, 64), (rrecv, rstage, 8)):
            lane = jnp.right_shift(iota((rows, 128), 1), 5)
            for u in range(2):
                blocks = [source[g, 4 * u + j].astype(F32) for j in range(4)]
                for a in range(4):
                    mine = [jnp.bitwise_and(lane - a, 3) == j for j in range(3)]
                    v = jnp.where(
                        mine[0], blocks[0], jnp.where(mine[1], blocks[1], jnp.where(mine[2], blocks[2], blocks[3]))
                    )
                    if a:
                        v = pltpu.roll(v, 128 - 32 * a, 1)
                    at = 256 * a + 128 * u
                    stage[g, :, at : at + 128] = v.astype(BF16)
        lanes = pl.ds(1024 * g, 1024)
        copies.append(pltpu.make_async_copy(ostage.at[g], out_s.at[:, lanes], sem.at[g]))
        copies.append(pltpu.make_async_copy(rstage.at[g], out_r.at[:, lanes], sem.at[4 + g]))
        for c in copies[-2:]:
            c.start()
    for c in copies:
        c.wait()


def solution(mesh):
    first, offset = trig_tables(128, 32, 64)

    def step(x, gain, w, rd, scal, look, payload, qn, qr):
        hbm = pl.BlockSpec(memory_space=pltpu.HBM)
        vmem = pl.BlockSpec(memory_space=pltpu.VMEM)
        dma = pltpu.SemaphoreType.DMA
        received = pl.pallas_call(
            kernel,
            out_shape=(
                jax.ShapeDtypeStruct((4, 8, 64, 128), BF16),
                jax.ShapeDtypeStruct((4, 8, 8, 128), BF16),
                jax.ShapeDtypeStruct((2, 128), BF16),
            ),
            in_specs=[hbm] * 11,
            out_specs=(vmem,) * 3,
            scratch_shapes=[
                pltpu.VMEM((16, 32, 2048), BF16),
                pltpu.VMEM((1, 2048), F32),
                pltpu.VMEM((2048, 512), BF16),
                pltpu.VMEM((64, 2048), BF16),
                pltpu.VMEM((1, 512), F32),
                pltpu.VMEM((1024, 128), BF16),
                pltpu.VMEM((1024, 128), BF16),
                pltpu.VMEM((136, 128), F32),
                pltpu.VMEM((32, 128), F32),
                pltpu.VMEM((16, 32, 640), BF16),
                pltpu.VMEM((16, 32, 640), BF16),
                pltpu.VMEM((8, 2, 128), BF16),
                pltpu.VMEM((8, 2, 64), BF16),
                pltpu.VMEM((8, 16, 128), BF16),
                pltpu.VMEM((8, 2, 64, 128), BF16),
                pltpu.VMEM((2, 512, 128), BF16),
                pltpu.VMEM((4, 8, 64, 128), BF16),
                pltpu.VMEM((4, 8, 8, 128), BF16),
                pltpu.VMEM((8, 2, 640), F32),
                pltpu.VMEM((8, 2, 640), F32),
                pltpu.VMEM((4, 16, 128), F32),
                dma((16,)),
                dma((10,)),
                dma((16,)),
                dma((16,)),
                dma((2, 8)),
                dma((2, 8)),
                dma((8,)),
                dma((8,)),
                dma((8,)),
                dma((8,)),
                dma((2, 4, 8)),
                dma((2, 4, 8)),
                dma((8,)),
                dma((8,)),
            ],
            compiler_params=pltpu.CompilerParams(
                collective_id=0, has_side_effects=True, vmem_limit_bytes=48 * 1024 * 1024
            ),
        )(
            *(
                pltpu.with_memory_space_constraint(v, pltpu.HBM)
                for v in (
                    x, gain.reshape(1, 2048), w, rd.T, scal.reshape(1, 512), look.reshape(1024, 128),
                    payload.reshape(1024, 128), qn.reshape(2, 128), qr.reshape(2, 64),
                    jnp.asarray(first), jnp.asarray(offset),
                )
            )
        )
        stored, rotary, read = pl.pallas_call(
            arrange,
            out_shape=(
                jax.ShapeDtypeStruct((64, 4096), BF16),
                jax.ShapeDtypeStruct((8, 4096), BF16),
                jax.ShapeDtypeStruct((2, 128), BF16),
            ),
            in_specs=[vmem] * 3,
            out_specs=(hbm,) * 3,
            scratch_shapes=[
                pltpu.VMEM((4, 64, 1024), BF16),
                pltpu.VMEM((4, 8, 1024), BF16),
                dma((9,)),
            ],
        )(*(pltpu.with_memory_space_constraint(v, pltpu.VMEM) for v in received))
        return stored.T[None], rotary.T[None], read[None]

    tp = "tp"
    both = ("sp", "tp")
    in_specs = (
        P(None, both, None), P(), P(), P(), P(), P(tp, None, None), P(tp, None, None),
        P("sp", tp, None), P("sp", tp, None),
    )
    out_specs = (P("sp", None, tp), P("sp", None, tp), P("sp", tp, None))
    return jax.shard_map(step, mesh=mesh, in_specs=in_specs, out_specs=out_specs, check_vma=False)
```

```python
import jax
import jax.numpy as jnp
import numpy as np
from jax import lax
from jax.experimental import pallas as pl
from jax.experimental.pallas import tpu as pltpu
from jax.sharding import PartitionSpec as P

MESH = pl.DeviceIdType.MESH
EPS = 1e-6
ROPE_BASE = 10000.0
F32 = jnp.float32
BF16 = jnp.bfloat16

NT = (((1,), (1,)), ((), ()))

STEPS = (
    (2, 2), (1, 2), (3, 2), (2, 1),
    (2, 3), (1, 1), (3, 3), (1, 3),
    (3, 1), (2, 0), (0, 2), (1, 0),
    (3, 0), (0, 1), (0, 3), (0, 0),
)


def trig_tables(blocks, rows, rope):
    half = rope // 2
    freq = 1.0 / ROPE_BASE ** (np.arange(half, dtype=np.float64) * 2.0 / rope)
    freq = np.concatenate([freq, freq])
    first = np.arange(blocks + 8, dtype=np.float64)[:, None] * rows * freq
    offset = np.arange(rows, dtype=np.float64)[:, None] * freq

    def both(angle):
        return np.concatenate([np.cos(angle), np.sin(angle)], axis=1).astype(np.float32)

    return both(first), both(offset)


def half_swap(v):
    half = v.shape[-1] // 2
    return jnp.concatenate([v[..., half:], v[..., :half]], axis=-1)


def iota(shape, dim):
    return lax.broadcasted_iota(jnp.int32, shape, dim)


def sp_at(sp, dz, dy):
    return lax.rem(sp // 4 + dz, 4) * 4 + lax.rem(lax.rem(sp, 4) + dy, 4)


def kernel(
    x_hbm, gain_hbm, w_hbm, rd_hbm, scal_hbm, look_hbm, pay_hbm, qn_hbm, qr_hbm, tab_hbm, off_hbm,
    krecv, rrecv, read_out,
    xb, gain, w, rd, scal, look, pay, tab, off,
    kst, rst, kall, rall, qn, qr, aall, pst, pall, ktst, rtst, asc, arecv,
    xsem, wsem, ksend, krsem, rsend, rrsem, qsend, qrsem, small, k2sem,
):
    sp, tp = lax.axis_index("sp"), lax.axis_index("tp")

    def tp_of(step):
        return lax.rem(tp + step, 8)

    for n in range(4):
        pltpu.make_async_copy(x_hbm.at[sp_at(sp, *STEPS[n])], xb.at[n], xsem.at[0]).start()
    halves = [pl.ds(0, 1024), pl.ds(1024, 1024)]
    loads = [
        pltpu.make_async_copy(src, dst, wsem.at[n])
        for n, (src, dst) in enumerate(
            (
                (gain_hbm, gain), (w_hbm.at[halves[0]], w.at[halves[0]]), (w_hbm.at[halves[1]], w.at[halves[1]]),
                (rd_hbm, rd), (scal_hbm, scal), (tab_hbm, tab), (off_hbm, off),
                (look_hbm, look), (pay_hbm, pay), (qn_hbm, qn.at[tp]), (qr_hbm, qr.at[tp]),
            )
        )
    ]
    for c in loads[:7]:
        c.start()

    barrier = pltpu.get_barrier_semaphore()

    def greet_sp(n, _):
        pl.semaphore_signal(barrier, inc=1, device_id=(lax.rem(sp + n, 16), tp), device_id_type=MESH)
        return 0

    def greet_tp(n, _):
        pl.semaphore_signal(barrier, inc=1, device_id=(sp, tp_of(n)), device_id_type=MESH)
        return 0

    lax.fori_loop(1, 16, greet_sp, 0)
    lax.fori_loop(1, 8, greet_tp, 0)

    def to_tp(src, dst, send, recv, step):
        return pltpu.make_async_remote_copy(
            src_ref=src, dst_ref=dst, send_sem=send, recv_sem=recv,
            device_id=(sp, tp_of(step)), device_id_type=MESH,
        )

    def to_all_tp(copies):
        def send(step, _):
            for c in copies(step):
                c.start()
            return 0

        lax.fori_loop(1, 8, send, 0)

    def to_sp(src, dst, send, recv, n):
        return pltpu.make_async_remote_copy(
            src_ref=src, dst_ref=dst, send_sem=send, recv_sem=recv,
            device_id=(sp_at(sp, *STEPS[n]), tp), device_id_type=MESH,
        )

    for c in loads[5:7]:
        c.wait()
    sign = jnp.where(iota((32, 64), 1) < 32, -1.0, 1.0).astype(F32)
    base = tab[pl.ds(sp * 8 + tp, 1), :]
    offs = off[...]
    cos = base[:, :64] * offs[:, :64] - base[:, 64:] * offs[:, 64:]
    sin = (base[:, 64:] * offs[:, :64] + base[:, :64] * offs[:, 64:]) * sign
    cos4 = jnp.concatenate([cos] * 4, axis=0)
    sin4 = jnp.concatenate([sin] * 4, axis=0)
    loads[0].wait()

    def project(k):
        pltpu.make_async_copy(x_hbm.at[pl.ds(0, 4)], xb.at[pl.ds(4 * k, 4)], xsem.at[k]).wait()
        xv = xb[4 * k : 4 * k + 4].reshape(128, 2048).astype(F32)
        scale = lax.rsqrt(jnp.mean(xv * xv, axis=1, keepdims=True) + EPS)
        normed = (xv * scale * gain[...]).astype(BF16)
        if k == 0:
            loads[1].wait()
        latent = jnp.dot(normed[:, :1024], w[:1024], preferred_element_type=F32)
        if k == 0:
            for c in loads[2:5]:
                c.wait()
            for n in range(4, 16):
                pltpu.make_async_copy(x_hbm.at[sp_at(sp, *STEPS[n])], xb.at[n], xsem.at[n // 4]).start()
            for c in loads[7:]:
                c.start()
        latent += jnp.dot(normed[:, 1024:], w[1024:], preferred_element_type=F32)
        latent = latent.astype(BF16).astype(F32)
        rot = lax.dot_general(normed, rd[...], NT, preferred_element_type=F32).astype(BF16).astype(F32)
        scale = lax.rsqrt(jnp.mean(latent * latent, axis=1, keepdims=True) + EPS)
        stored = (latent * scale * scal[...]).astype(BF16).reshape(4, 32, 512)
        turned = (rot * cos4 + half_swap(rot) * sin4).reshape(4, 2, 16, 64)
        turned = jnp.concatenate([turned[:, 0], turned[:, 1]], axis=-1).astype(BF16)
        kst[4 * k : 4 * k + 4] = stored
        rst[4 * k : 4 * k + 4] = turned
        if k == 3:
            kall[12 + lax.rem(3 + tp, 4)] = stored[3]
            rall[12 + lax.rem(3 + tp, 4)] = turned[3]
        if k == 0:
            pl.semaphore_wait(barrier, 22)
        for n in range(4 * k, min(4 * k + 4, 15)):
            slot = 4 * k + lax.rem(n + tp, 4)
            to_sp(kst.at[n], kall.at[slot], ksend, krsem.at[k], n).start()
            to_sp(rst.at[n], rall.at[slot], rsend, rrsem.at[k], n).start()

    def arrived(k):
        count = 4 if k < 3 else 3
        at = pl.ds(4 * k, count)
        to_sp(kst.at[at], kall.at[at], ksend, krsem.at[k], 0).wait_recv()
        to_sp(rst.at[at], rall.at[at], rsend, rrsem.at[k], 0).wait_recv()

    project(0)
    to_all_tp(
        lambda step: (
            to_tp(qn_hbm, qn.at[tp], qsend.at[0], qrsem.at[0], step),
            to_tp(qr_hbm, qr.at[tp], qsend.at[1], qrsem.at[1], step),
        )
    )

    loads[8].wait()
    row, col = iota((256, 256), 0), iota((256, 256), 1)
    wanted = jnp.bitwise_and(row, 15) * 16 + jnp.right_shift(row, 4)
    order = jnp.where(col == wanted, 1.0, 0.0).astype(BF16)
    for g in range(4):
        rows = jnp.dot(order, pay[256 * g : 256 * (g + 1), :], preferred_element_type=F32)
        pst[:, :, 16 * g : 16 * (g + 1), :] = rows.astype(BF16).reshape(8, 2, 16, 128)
    mine = pl.ds(pl.multiple_of(tp * 64, 64), 64)
    pall[:, mine, :] = pst[tp]
    to_all_tp(lambda step: (to_tp(pst.at[tp_of(step)], pall.at[:, mine, :], small.at[0], small.at[1], step),))

    project(1)
    project(2)

    for n in (7, 9, 10):
        loads[n].wait()
    seven = pl.ds(0, 7)
    to_tp(qn.at[seven], qn.at[seven], qsend.at[0], qrsem.at[0], 1).wait_recv()
    to_tp(qr.at[seven], qr.at[seven], qsend.at[1], qrsem.at[1], 1).wait_recv()
    q_all = qn[...].astype(F32).reshape(16, 128).astype(BF16)
    t_all = qr[...].astype(F32).reshape(16, 64)
    parts = lax.dot_general(q_all, look[...], NT, preferred_element_type=F32)
    same = jnp.bitwise_and(iota((16, 1024), 1), 15) == iota((16, 1024), 0)
    parts = jnp.where(same, parts, 0.0).astype(BF16)
    pick = jnp.right_shift(iota((1024, 128), 0), 4) + 64 * lax.rem(tp, 2) == iota((1024, 128), 1)
    pick = jnp.where(pick, 1.0, 0.0).astype(BF16)
    aall[tp] = jnp.dot(parts, pick, preferred_element_type=F32).astype(BF16)
    to_all_tp(lambda step: (to_tp(aall.at[tp], aall.at[tp], small.at[2], small.at[3], step),))
    last = tab[128:129, :]
    q_turn = (t_all * last[:, :64] + half_swap(t_all) * (last[:, 64:] * sign[:1])).astype(BF16)

    project(3)

    def keys(k):
        packed = rall[4 * k : 4 * k + 4].astype(F32)
        swapped = half_swap(packed)
        rows = jnp.concatenate([packed[:, None, :, :64], swapped[:, None, :, :64]], axis=1)
        return rows.reshape(128, 64)

    def spread(k, rows):
        ktst[k] = kall[4 * k : 4 * k + 4].reshape(128, 512).T.reshape(8, 64, 128)
        rtst[k] = rows.T.reshape(8, 8, 128).astype(BF16)
        to_all_tp(
            lambda step: (
                to_tp(ktst.at[k, tp_of(step)], krecv.at[k, tp], k2sem.at[0], k2sem.at[1], step),
                to_tp(rtst.at[k, tp_of(step)], rrecv.at[k, tp], k2sem.at[2], k2sem.at[3], step),
            )
        )
        krecv[k, tp] = ktst[k, tp]
        rrecv[k, tp] = rtst[k, tp]

    rows = []
    for k in range(3):
        arrived(k)
        rows.append(keys(k))
        spread(k, rows[k])

    to_tp(aall.at[seven], aall.at[seven], small.at[2], small.at[3], 1).wait_recv()
    absorbed = jnp.concatenate([aall[2 * u] + aall[2 * u + 1] for u in range(4)], axis=1)

    def scores(k, rows):
        latent = kall[4 * k : 4 * k + 4].reshape(128, 512)
        total = lax.dot_general(absorbed, latent, NT, preferred_element_type=F32)
        total += lax.dot_general(q_turn, rows.astype(BF16), NT, preferred_element_type=F32)
        return total * (192.0 ** -0.5)

    def mixed(weight, k):
        latent = kall[4 * k : 4 * k + 4].reshape(128, 512)
        return jnp.dot(weight.astype(BF16), latent, preferred_element_type=F32)

    seen = [scores(k, rows[k]) for k in range(3)]
    top_seen = jnp.max(jnp.maximum(jnp.maximum(seen[0], seen[1]), seen[2]), axis=1, keepdims=True)
    weights = [jnp.exp(s - top_seen) for s in seen]
    total_seen = jnp.sum(weights[0] + weights[1] + weights[2], axis=1, keepdims=True)
    context_seen = mixed(weights[0], 0) + mixed(weights[1], 1) + mixed(weights[2], 2)

    arrived(3)
    last_rows = keys(3)
    late = scores(3, last_rows)
    top = jnp.maximum(top_seen, jnp.max(late, axis=1, keepdims=True))
    weight = jnp.exp(late - top)
    shrink = jnp.exp(top_seen - top)
    total = total_seen * shrink + jnp.sum(weight, axis=1, keepdims=True)
    context = context_seen * shrink + mixed(weight, 3)
    stats = jnp.where(iota((16, 128), 1) < 64, top, total)
    for t in range(8):
        asc[t, :, :512] = context[2 * t : 2 * t + 2]
        asc[t, :, 512:] = stats[2 * t : 2 * t + 2]
    to_all_tp(lambda step: (to_tp(asc.at[tp_of(step)], arecv.at[tp], small.at[4], small.at[5], step),))
    arecv[tp] = asc[tp]
    spread(3, last_rows)

    to_tp(pst.at[seven], pst.at[seven], small.at[0], small.at[1], 1).wait_recv()
    to_tp(asc.at[seven], arecv.at[seven], small.at[4], small.at[5], 1).wait_recv()
    got = arecv[...]
    tops, totals = got[:, :, 512:513], got[:, :, 576:577]
    share = jnp.exp(tops - jnp.max(tops, axis=0, keepdims=True))
    summed = jnp.sum(got[:, :, :512] * share, axis=0) / jnp.sum(totals * share, axis=0)
    summed = jnp.concatenate([summed, jnp.zeros((14, 512), F32)], axis=0).astype(BF16)
    first = jnp.dot(summed, pall[0], preferred_element_type=F32)
    second = jnp.dot(summed, pall[1], preferred_element_type=F32)
    values = jnp.where(iota((16, 128), 0) == 0, first, second)[:2]
    values = values * lax.rsqrt(jnp.mean(values * values, axis=1, keepdims=True) + EPS)
    read_out[...] = values.astype(BF16)

    sent = pl.ds(0, 15)
    to_sp(kst.at[sent], kall.at[sent], ksend, krsem.at[0], 0).wait_send()
    to_sp(rst.at[sent], rall.at[sent], rsend, rrsem.at[0], 0).wait_send()
    to_tp(qn.at[seven], qn.at[seven], qsend.at[0], qrsem.at[0], 1).wait_send()
    to_tp(qr.at[seven], qr.at[seven], qsend.at[1], qrsem.at[1], 1).wait_send()
    to_tp(pst.at[seven], pst.at[seven], small.at[0], small.at[1], 1).wait_send()
    to_tp(aall.at[seven], aall.at[seven], small.at[2], small.at[3], 1).wait_send()
    to_tp(asc.at[seven], arecv.at[seven], small.at[4], small.at[5], 1).wait_send()
    blocks = to_tp(ktst.at[:, seven], krecv.at[:, seven], k2sem.at[0], k2sem.at[1], 1)
    turned = to_tp(rtst.at[:, seven], rrecv.at[:, seven], k2sem.at[2], k2sem.at[3], 1)
    for c in (blocks, turned):
        c.wait_send()
        c.wait_recv()


def arrange(krecv, rrecv, read_in, out_s, out_r, out_f, stage, turned_stage, sem):
    sp = lax.axis_index("sp")
    read = pltpu.make_async_copy(read_in, out_f, sem.at[2])
    read.start()
    for k in range(4):
        at = [256 * sp_at(sp, (4 - dz) % 4, (4 - dy) % 4) for dz, dy in STEPS[4 * k : 4 * k + 4]]
        for source, held, rows in ((krecv, stage, 64), (rrecv, turned_stage, 8)):
            lane = jnp.right_shift(iota((rows, 128), 1), 5)
            for u in range(2):
                blocks = [source[k, 4 * u + j].astype(F32) for j in range(4)]
                for a in range(4):
                    mine = [jnp.bitwise_and(lane - a, 3) == j for j in range(3)]
                    v = jnp.where(
                        mine[0], blocks[0], jnp.where(mine[1], blocks[1], jnp.where(mine[2], blocks[2], blocks[3]))
                    )
                    if a:
                        v = pltpu.roll(v, 128 - 32 * a, 1)
                    held[:, pl.ds(pl.multiple_of(at[a] + 128 * u, 128), 128)] = v.astype(BF16)
        for a in range(4):
            lanes = pl.ds(pl.multiple_of(at[a], 256), 256)
            pltpu.make_async_copy(stage.at[:, lanes], out_s.at[:, lanes], sem.at[0]).start()
    turned = pltpu.make_async_copy(turned_stage, out_r, sem.at[1])
    turned.start()
    pltpu.make_async_copy(stage, out_s, sem.at[0]).wait()
    turned.wait()
    read.wait()


def solution(mesh):
    first, offset = trig_tables(128, 32, 64)

    def step(x, gain, w, rd, scal, look, payload, qn, qr):
        hbm = pl.BlockSpec(memory_space=pltpu.HBM)
        vmem = pl.BlockSpec(memory_space=pltpu.VMEM)
        dma = pltpu.SemaphoreType.DMA
        received = pl.pallas_call(
            kernel,
            out_shape=(
                jax.ShapeDtypeStruct((4, 8, 64, 128), BF16),
                jax.ShapeDtypeStruct((4, 8, 8, 128), BF16),
                jax.ShapeDtypeStruct((2, 128), BF16),
            ),
            in_specs=[hbm] * 11,
            out_specs=(vmem,) * 3,
            scratch_shapes=[
                pltpu.VMEM((16, 32, 2048), BF16),
                pltpu.VMEM((1, 2048), F32),
                pltpu.VMEM((2048, 512), BF16),
                pltpu.VMEM((64, 2048), BF16),
                pltpu.VMEM((1, 512), F32),
                pltpu.VMEM((1024, 128), BF16),
                pltpu.VMEM((1024, 128), BF16),
                pltpu.VMEM((136, 128), F32),
                pltpu.VMEM((32, 128), F32),
                pltpu.VMEM((16, 32, 512), BF16),
                pltpu.VMEM((16, 16, 128), BF16),
                pltpu.VMEM((16, 32, 512), BF16),
                pltpu.VMEM((16, 16, 128), BF16),
                pltpu.VMEM((8, 2, 128), BF16),
                pltpu.VMEM((8, 2, 64), BF16),
                pltpu.VMEM((8, 16, 128), BF16),
                pltpu.VMEM((8, 2, 64, 128), BF16),
                pltpu.VMEM((2, 512, 128), BF16),
                pltpu.VMEM((4, 8, 64, 128), BF16),
                pltpu.VMEM((4, 8, 8, 128), BF16),
                pltpu.VMEM((8, 2, 640), F32),
                pltpu.VMEM((8, 2, 640), F32),
                dma((4,)),
                dma((11,)),
                dma,
                dma((4,)),
                dma,
                dma((4,)),
                dma((2,)),
                dma((2,)),
                dma((6,)),
                dma((4,)),
            ],
            compiler_params=pltpu.CompilerParams(
                collective_id=0, has_side_effects=True, vmem_limit_bytes=48 * 1024 * 1024
            ),
        )(
            *(
                pltpu.with_memory_space_constraint(v, pltpu.HBM)
                for v in (
                    x, gain.reshape(1, 2048), w, rd.T, scal.reshape(1, 512), look.reshape(1024, 128),
                    payload.reshape(1024, 128), qn.reshape(2, 128), qr.reshape(2, 64),
                    jnp.asarray(first), jnp.asarray(offset),
                )
            )
        )
        stored, rotary, read = pl.pallas_call(
            arrange,
            out_shape=(
                jax.ShapeDtypeStruct((64, 4096), BF16),
                jax.ShapeDtypeStruct((8, 4096), BF16),
                jax.ShapeDtypeStruct((2, 128), BF16),
            ),
            in_specs=[vmem] * 3,
            out_specs=(hbm,) * 3,
            scratch_shapes=[
                pltpu.VMEM((64, 4096), BF16),
                pltpu.VMEM((8, 4096), BF16),
                dma((3,)),
            ],
        )(*(pltpu.with_memory_space_constraint(v, pltpu.VMEM) for v in received))
        return stored.T[None], rotary.T[None], read[None]

    tp = "tp"
    both = ("sp", "tp")
    in_specs = (
        P(None, both, None), P(), P(), P(), P(), P(tp, None, None), P(tp, None, None),
        P("sp", tp, None), P("sp", tp, None),
    )
    out_specs = (P("sp", None, tp), P("sp", None, tp), P("sp", tp, None))
    return jax.shard_map(step, mesh=mesh, in_specs=in_specs, out_specs=out_specs, check_vma=False)
```

```python
import jax
import jax.numpy as jnp
import numpy as np
from jax import lax
from jax.experimental import pallas as pl
from jax.experimental.pallas import tpu as pltpu
from jax.sharding import PartitionSpec as P

MESH = pl.DeviceIdType.MESH
EPS = 1e-6
ROPE_BASE = 10000.0
F32 = jnp.float32
BF16 = jnp.bfloat16

NT = (((1,), (1,)), ((), ()))

STEPS = (
    (1, 1), (3, 3), (2, 0), (0, 2),
    (1, 3), (3, 1), (1, 2), (3, 2),
    (2, 1), (2, 3), (1, 0), (3, 0),
    (0, 1), (0, 3), (2, 2), (0, 0),
)
OWN = STEPS.index((0, 0))
OTHERS = 1 if OWN == 0 else 0


def trig_tables(blocks, rows, rope):
    half = rope // 2
    freq = 1.0 / ROPE_BASE ** (np.arange(half, dtype=np.float64) * 2.0 / rope)
    freq = np.concatenate([freq, freq])
    first = np.arange(blocks + 8, dtype=np.float64)[:, None] * rows * freq
    offset = np.arange(rows, dtype=np.float64)[:, None] * freq

    def both(angle):
        return np.concatenate([np.cos(angle), np.sin(angle)], axis=1).astype(np.float32)

    return both(first), both(offset)


def half_swap(v):
    half = v.shape[-1] // 2
    return jnp.concatenate([v[..., half:], v[..., :half]], axis=-1)


def iota(shape, dim):
    return lax.broadcasted_iota(jnp.int32, shape, dim)


def sp_at(sp, dz, dy):
    return lax.rem(sp // 4 + dz, 4) * 4 + lax.rem(lax.rem(sp, 4) + dy, 4)


def kernel(
    x_hbm, gain_hbm, w_hbm, rd_hbm, scal_hbm, look_hbm, pay_hbm, qn_hbm, qr_hbm, tab_hbm, off_hbm,
    krecv, rrecv, read_out,
    xb, gain, w, rd, scal, look, pay, tab, off,
    kst, rst, kall, rall, qn, qr, aall, pst, pall, ktst, rtst, asc, arecv, order, part, held,
    xsem, wsem, ksend, krsem, rsend, rrsem, qsend, qrsem, small, k2sem,
):
    sp, tp = lax.axis_index("sp"), lax.axis_index("tp")

    def tp_of(step):
        return lax.rem(tp + step, 8)

    halves = [pl.ds(0, 1024), pl.ds(1024, 1024)]
    loads = [
        pltpu.make_async_copy(src, dst, wsem.at[n])
        for n, (src, dst) in enumerate(
            (
                (gain_hbm, gain), (w_hbm.at[halves[0]], w.at[halves[0], pl.ds(0, 512)]),
                (w_hbm.at[halves[1]], w.at[halves[1], pl.ds(0, 512)]),
                (rd_hbm, rd), (scal_hbm, scal), (tab_hbm, tab), (off_hbm, off),
                (look_hbm, look), (pay_hbm, pay), (qn_hbm, qn.at[tp]), (qr_hbm, qr.at[tp]),
            )
        )
    ]
    for n in (5, 6, 0, 3):
        loads[n].start()
    for n in range(4):
        pltpu.make_async_copy(x_hbm.at[sp_at(sp, *STEPS[n])], xb.at[n], xsem.at[0]).start()
    loads[1].start()

    barrier = pltpu.get_barrier_semaphore()
    for dz, dy in sorted(STEPS, key=lambda s: -min(s[0], 4 - s[0]) - min(s[1], 4 - s[1]))[:15]:
        pl.semaphore_signal(barrier, inc=1, device_id=(sp_at(sp, dz, dy), tp), device_id_type=MESH)
    for step in (4, 5, 3, 2, 6, 7, 1):
        pl.semaphore_signal(barrier, inc=1, device_id=(sp, tp_of(step)), device_id_type=MESH)

    for n in (4, 2):
        loads[n].start()

    def to_tp(src, dst, send, recv, step):
        return pltpu.make_async_remote_copy(
            src_ref=src, dst_ref=dst, send_sem=send, recv_sem=recv,
            device_id=(sp, tp_of(step)), device_id_type=MESH,
        )

    def to_all_tp(copies):
        def send(step, _):
            for c in copies(step):
                c.start()
            return 0

        lax.fori_loop(1, 8, send, 0)

    def to_sp(src, dst, send, recv, n):
        return pltpu.make_async_remote_copy(
            src_ref=src, dst_ref=dst, send_sem=send, recv_sem=recv,
            device_id=(sp_at(sp, *STEPS[n]), tp), device_id_type=MESH,
        )

    for c in loads[5:7]:
        c.wait()
    sign = jnp.where(iota((32, 64), 1) < 32, -1.0, 1.0).astype(F32)
    base = tab[pl.ds(sp * 8 + tp, 1), :]
    offs = off[...]
    cos = base[:, :64] * offs[:, :64] - base[:, 64:] * offs[:, 64:]
    sin = (base[:, 64:] * offs[:, :64] + base[:, :64] * offs[:, 64:]) * sign
    loads[0].wait()

    row, col = iota((256, 256), 0), iota((256, 256), 1)
    wanted = jnp.bitwise_and(row, 15) * 16 + jnp.right_shift(row, 4)
    order[...] = jnp.where(col == wanted, 1.0, 0.0).astype(BF16)
    loads[3].wait()
    w[:, 512:] = jnp.concatenate([rd[...].T, jnp.zeros((2048, 64), BF16)], axis=1)

    def project(k, groups):
        count = 4 * groups
        for n in range(groups):
            at = pl.ds(4 * (k + n), 4)
            pltpu.make_async_copy(x_hbm.at[pl.ds(0, 4)], xb.at[at], xsem.at[k + n]).wait()
        xv = xb[4 * k : 4 * k + count].reshape(32 * count, 2048).astype(F32)
        scale = lax.rsqrt(jnp.mean(xv * xv, axis=1, keepdims=True) + EPS)
        normed = (xv * scale * gain[...]).astype(BF16)
        if k == 0:
            rot = jnp.dot(normed, w[:, 512:], preferred_element_type=F32)
        else:
            both = jnp.dot(normed, w[...], preferred_element_type=F32)
            latent, rot = both[:, :512], both[:, 512:]
        rot = rot[:, :64].astype(BF16).astype(F32)
        turn = [jnp.concatenate([part] * count, axis=0) for part in (cos, sin)]
        turned = (rot * turn[0] + half_swap(rot) * turn[1]).reshape(count, 2, 16, 64)
        turned = jnp.concatenate([turned[:, 0], turned[:, 1]], axis=-1).astype(BF16)
        rst[4 * k : 4 * k + count] = turned
        if k == 0:
            loads[1].wait()
            for n in range(4, 8):
                pltpu.make_async_copy(x_hbm.at[sp_at(sp, *STEPS[n])], xb.at[n], xsem.at[n // 4]).start()
            part[...] = jnp.dot(normed[:, :1024], w[:1024, :512], preferred_element_type=F32)
            held[...] = normed

            @pl.when(sp >= 0)
            def _():
                for n in (2, 4):
                    loads[n].wait()
                for n in (8, 9, 10, 7):
                    loads[n].start()
                for n in range(8, 16):
                    pltpu.make_async_copy(x_hbm.at[sp_at(sp, *STEPS[n])], xb.at[n], xsem.at[n // 4]).start()

            normed = held[...]
            latent = part[...] + jnp.dot(normed[:, 1024:], w[1024:, :512], preferred_element_type=F32)
        latent = latent.astype(BF16).astype(F32)
        scale = lax.rsqrt(jnp.mean(latent * latent, axis=1, keepdims=True) + EPS)
        stored = (latent * scale * scal[...]).astype(BF16).reshape(count, 32, 512)
        kst[4 * k : 4 * k + count] = stored
        if 4 * k <= OWN < 4 * k + count:
            slot = OWN // 4 * 4 + lax.rem(OWN + tp, 4)
            kall[slot] = stored[OWN - 4 * k]
            rall[slot] = rst[OWN]
        if k == 0:
            pl.semaphore_wait(barrier, 22)
        for n in range(4 * k, 4 * k + count):
            if n != OWN:
                slot = n // 4 * 4 + lax.rem(n + tp, 4)
                to_sp(kst.at[n], kall.at[slot], ksend, krsem.at[n // 4], n).start()
                to_sp(rst.at[n], rall.at[slot], rsend, rrsem.at[n // 4], n).start()

    def arrived(k):
        count = 4 if k != OWN // 4 else 3
        at = pl.ds(4 * k, count)
        to_sp(kst.at[at], kall.at[at], ksend, krsem.at[k], OTHERS).wait_recv()
        to_sp(rst.at[at], rall.at[at], rsend, rrsem.at[k], OTHERS).wait_recv()

    project(0, 1)
    to_all_tp(
        lambda step: (
            to_tp(qn_hbm, qn.at[tp], qsend.at[0], qrsem.at[0], step),
            to_tp(qr_hbm, qr.at[tp], qsend.at[1], qrsem.at[1], step),
        )
    )

    project(1, 1)

    loads[8].wait()
    for g in range(4):
        rows = jnp.dot(order[...], pay[256 * g : 256 * (g + 1), :], preferred_element_type=F32)
        pst[:, :, 16 * g : 16 * (g + 1), :] = rows.astype(BF16).reshape(8, 2, 16, 128)
    mine = pl.ds(pl.multiple_of(tp * 64, 64), 64)
    pall[:, mine, :] = pst[tp]
    to_all_tp(lambda step: (to_tp(pst.at[tp_of(step)], pall.at[:, mine, :], small.at[0], small.at[1], step),))

    project(2, 1)
    project(3, 1)

    for n in (7, 9, 10):
        loads[n].wait()
    seven = pl.ds(0, 7)
    to_tp(qn.at[seven], qn.at[seven], qsend.at[0], qrsem.at[0], 1).wait_recv()
    to_tp(qr.at[seven], qr.at[seven], qsend.at[1], qrsem.at[1], 1).wait_recv()
    q_all = qn[...].astype(F32).reshape(16, 128).astype(BF16)
    t_all = qr[...].astype(F32).reshape(16, 64)
    parts = lax.dot_general(q_all, look[...], NT, preferred_element_type=F32)
    same = jnp.bitwise_and(iota((16, 1024), 1), 15) == iota((16, 1024), 0)
    parts = jnp.where(same, parts, 0.0).astype(BF16)
    pick = jnp.right_shift(iota((1024, 128), 0), 4) + 64 * lax.rem(tp, 2) == iota((1024, 128), 1)
    pick = jnp.where(pick, 1.0, 0.0).astype(BF16)
    aall[tp] = jnp.dot(parts, pick, preferred_element_type=F32).astype(BF16)
    to_all_tp(lambda step: (to_tp(aall.at[tp], aall.at[tp], small.at[2], small.at[3], step),))
    last = tab[128:129, :]
    q_turn = (t_all * last[:, :64] + half_swap(t_all) * (last[:, 64:] * sign[:1])).astype(BF16)

    def keys(k):
        packed = rall[4 * k : 4 * k + 4].astype(F32)
        swapped = half_swap(packed)
        rows = jnp.concatenate([packed[:, None, :, :64], swapped[:, None, :, :64]], axis=1)
        return rows.reshape(128, 64)

    def spread(k, rows):
        ktst[k] = kall[4 * k : 4 * k + 4].reshape(128, 512).T.reshape(8, 64, 128)
        rtst[k] = rows.T.reshape(8, 8, 128).astype(BF16)
        to_all_tp(
            lambda step: (
                to_tp(ktst.at[k, tp_of(step)], krecv.at[k, tp], k2sem.at[0], k2sem.at[1], step),
                to_tp(rtst.at[k, tp_of(step)], rrecv.at[k, tp], k2sem.at[2], k2sem.at[3], step),
            )
        )
        krecv[k, tp] = ktst[k, tp]
        rrecv[k, tp] = rtst[k, tp]

    rows = []
    for k in range(3):
        arrived(k)
        rows.append(keys(k))
        spread(k, rows[k])

    to_tp(aall.at[seven], aall.at[seven], small.at[2], small.at[3], 1).wait_recv()
    absorbed = jnp.concatenate([aall[2 * u] + aall[2 * u + 1] for u in range(4)], axis=1)

    def scores(k, rows):
        latent = kall[4 * k : 4 * k + 4].reshape(128, 512)
        total = lax.dot_general(absorbed, latent, NT, preferred_element_type=F32)
        total += lax.dot_general(q_turn, rows.astype(BF16), NT, preferred_element_type=F32)
        return total * (192.0 ** -0.5)

    def mixed(weight, k):
        latent = kall[4 * k : 4 * k + 4].reshape(128, 512)
        return jnp.dot(weight.astype(BF16), latent, preferred_element_type=F32)

    seen = [scores(k, rows[k]) for k in range(3)]
    top_seen = jnp.max(jnp.maximum(jnp.maximum(seen[0], seen[1]), seen[2]), axis=1, keepdims=True)
    weights = [jnp.exp(s - top_seen) for s in seen]
    total_seen = jnp.sum(weights[0] + weights[1] + weights[2], axis=1, keepdims=True)
    context_seen = mixed(weights[0], 0) + mixed(weights[1], 1) + mixed(weights[2], 2)

    arrived(3)
    last_rows = keys(3)
    late = scores(3, last_rows)
    top = jnp.maximum(top_seen, jnp.max(late, axis=1, keepdims=True))
    weight = jnp.exp(late - top)
    shrink = jnp.exp(top_seen - top)
    total = total_seen * shrink + jnp.sum(weight, axis=1, keepdims=True)
    context = context_seen * shrink + mixed(weight, 3)
    stats = jnp.where(iota((16, 128), 1) < 64, top, total)
    for t in range(8):
        asc[t, :, :512] = context[2 * t : 2 * t + 2]
        asc[t, :, 512:] = stats[2 * t : 2 * t + 2]
    to_all_tp(lambda step: (to_tp(asc.at[tp_of(step)], arecv.at[tp], small.at[4], small.at[5], step),))
    arecv[tp] = asc[tp]
    spread(3, last_rows)

    to_tp(pst.at[seven], pst.at[seven], small.at[0], small.at[1], 1).wait_recv()
    to_tp(asc.at[seven], arecv.at[seven], small.at[4], small.at[5], 1).wait_recv()
    got = arecv[...]
    tops, totals = got[:, :, 512:513], got[:, :, 576:577]
    share = jnp.exp(tops - jnp.max(tops, axis=0, keepdims=True))
    summed = jnp.sum(got[:, :, :512] * share, axis=0) / jnp.sum(totals * share, axis=0)
    summed = jnp.concatenate([summed, jnp.zeros((14, 512), F32)], axis=0).astype(BF16)
    first = jnp.dot(summed, pall[0], preferred_element_type=F32)
    second = jnp.dot(summed, pall[1], preferred_element_type=F32)
    values = jnp.where(iota((16, 128), 0) == 0, first, second)[:2]
    values = values * lax.rsqrt(jnp.mean(values * values, axis=1, keepdims=True) + EPS)
    read_out[...] = values.astype(BF16)

    sent = pl.ds(OTHERS, 15)
    to_sp(kst.at[sent], kall.at[sent], ksend, krsem.at[0], OTHERS).wait_send()
    to_sp(rst.at[sent], rall.at[sent], rsend, rrsem.at[0], OTHERS).wait_send()
    to_tp(qn.at[seven], qn.at[seven], qsend.at[0], qrsem.at[0], 1).wait_send()
    to_tp(qr.at[seven], qr.at[seven], qsend.at[1], qrsem.at[1], 1).wait_send()
    to_tp(pst.at[seven], pst.at[seven], small.at[0], small.at[1], 1).wait_send()
    to_tp(aall.at[seven], aall.at[seven], small.at[2], small.at[3], 1).wait_send()
    to_tp(asc.at[seven], arecv.at[seven], small.at[4], small.at[5], 1).wait_send()
    blocks = to_tp(ktst.at[:, seven], krecv.at[:, seven], k2sem.at[0], k2sem.at[1], 1)
    turned = to_tp(rtst.at[:, seven], rrecv.at[:, seven], k2sem.at[2], k2sem.at[3], 1)
    for c in (blocks, turned):
        c.wait_send()
        c.wait_recv()


def arrange(krecv, rrecv, read_in, out_s, out_r, out_f, stage, turned_stage, sem):
    sp = lax.axis_index("sp")
    read = pltpu.make_async_copy(read_in, out_f, sem.at[2])
    read.start()
    for k in range(4):
        at = [256 * sp_at(sp, (4 - dz) % 4, (4 - dy) % 4) for dz, dy in STEPS[4 * k : 4 * k + 4]]
        for source, held, rows in ((krecv, stage, 64), (rrecv, turned_stage, 8)):
            lane = jnp.right_shift(iota((rows, 128), 1), 5)
            for u in range(2):
                blocks = [source[k, 4 * u + j].astype(F32) for j in range(4)]
                for a in range(4):
                    mine = [jnp.bitwise_and(lane - a, 3) == j for j in range(3)]
                    v = jnp.where(
                        mine[0], blocks[0], jnp.where(mine[1], blocks[1], jnp.where(mine[2], blocks[2], blocks[3]))
                    )
                    if a:
                        v = pltpu.roll(v, 128 - 32 * a, 1)
                    held[:, pl.ds(pl.multiple_of(at[a] + 128 * u, 128), 128)] = v.astype(BF16)
        for a in range(4):
            lanes = pl.ds(pl.multiple_of(at[a], 256), 256)
            pltpu.make_async_copy(stage.at[:, lanes], out_s.at[:, lanes], sem.at[0]).start()
    turned = pltpu.make_async_copy(turned_stage, out_r, sem.at[1])
    turned.start()
    pltpu.make_async_copy(stage, out_s, sem.at[0]).wait()
    turned.wait()
    read.wait()


def solution(mesh):
    first, offset = trig_tables(128, 32, 64)

    def step(x, gain, w, rd, scal, look, payload, qn, qr):
        hbm = pl.BlockSpec(memory_space=pltpu.HBM)
        vmem = pl.BlockSpec(memory_space=pltpu.VMEM)
        dma = pltpu.SemaphoreType.DMA
        received = pl.pallas_call(
            kernel,
            out_shape=(
                jax.ShapeDtypeStruct((4, 8, 64, 128), BF16),
                jax.ShapeDtypeStruct((4, 8, 8, 128), BF16),
                jax.ShapeDtypeStruct((2, 128), BF16),
            ),
            in_specs=[hbm] * 11,
            out_specs=(vmem,) * 3,
            scratch_shapes=[
                pltpu.VMEM((16, 32, 2048), BF16),
                pltpu.VMEM((1, 2048), F32),
                pltpu.VMEM((2048, 640), BF16),
                pltpu.VMEM((64, 2048), BF16),
                pltpu.VMEM((1, 512), F32),
                pltpu.VMEM((1024, 128), BF16),
                pltpu.VMEM((1024, 128), BF16),
                pltpu.VMEM((136, 128), F32),
                pltpu.VMEM((32, 128), F32),
                pltpu.VMEM((16, 32, 512), BF16),
                pltpu.VMEM((16, 16, 128), BF16),
                pltpu.VMEM((16, 32, 512), BF16),
                pltpu.VMEM((16, 16, 128), BF16),
                pltpu.VMEM((8, 2, 128), BF16),
                pltpu.VMEM((8, 2, 64), BF16),
                pltpu.VMEM((8, 16, 128), BF16),
                pltpu.VMEM((8, 2, 64, 128), BF16),
                pltpu.VMEM((2, 512, 128), BF16),
                pltpu.VMEM((4, 8, 64, 128), BF16),
                pltpu.VMEM((4, 8, 8, 128), BF16),
                pltpu.VMEM((8, 2, 640), F32),
                pltpu.VMEM((8, 2, 640), F32),
                pltpu.VMEM((256, 256), BF16),
                pltpu.VMEM((128, 512), F32),
                pltpu.VMEM((128, 2048), BF16),
                dma((4,)),
                dma((11,)),
                dma,
                dma((4,)),
                dma,
                dma((4,)),
                dma((2,)),
                dma((2,)),
                dma((6,)),
                dma((4,)),
            ],
            compiler_params=pltpu.CompilerParams(
                collective_id=0, has_side_effects=True, vmem_limit_bytes=48 * 1024 * 1024
            ),
        )(
            *(
                pltpu.with_memory_space_constraint(v, pltpu.HBM)
                for v in (
                    x, gain.reshape(1, 2048), w, rd.T, scal.reshape(1, 512), look.reshape(1024, 128),
                    payload.reshape(1024, 128), qn.reshape(2, 128), qr.reshape(2, 64),
                    jnp.asarray(first), jnp.asarray(offset),
                )
            )
        )
        stored, rotary, read = pl.pallas_call(
            arrange,
            out_shape=(
                jax.ShapeDtypeStruct((64, 4096), BF16),
                jax.ShapeDtypeStruct((8, 4096), BF16),
                jax.ShapeDtypeStruct((2, 128), BF16),
            ),
            in_specs=[vmem] * 3,
            out_specs=(hbm,) * 3,
            scratch_shapes=[
                pltpu.VMEM((64, 4096), BF16),
                pltpu.VMEM((8, 4096), BF16),
                dma((3,)),
            ],
        )(*(pltpu.with_memory_space_constraint(v, pltpu.VMEM) for v in received))
        return stored.T[None], rotary.T[None], read[None]

    tp = "tp"
    both = ("sp", "tp")
    in_specs = (
        P(None, both, None), P(), P(), P(), P(), P(tp, None, None), P(tp, None, None),
        P("sp", tp, None), P("sp", tp, None),
    )
    out_specs = (P("sp", None, tp), P("sp", None, tp), P("sp", tp, None))
    return jax.shard_map(step, mesh=mesh, in_specs=in_specs, out_specs=out_specs, check_vma=False)
```

```python
import jax
import jax.numpy as jnp
import numpy as np
from jax import lax
from jax.experimental import pallas as pl
from jax.experimental.pallas import tpu as pltpu
from jax.sharding import PartitionSpec as P

MESH = pl.DeviceIdType.MESH
EPS = 1e-6
ROPE_BASE = 10000.0
F32 = jnp.float32
BF16 = jnp.bfloat16

NT = (((1,), (1,)), ((), ()))

STEPS = (
    (1, 1), (3, 3), (2, 0), (0, 2),
    (1, 3), (3, 1), (1, 2), (3, 2),
    (2, 1), (2, 3), (1, 0), (3, 0),
    (0, 1), (0, 3), (2, 2), (0, 0),
)
OWN = STEPS.index((0, 0))
OTHERS = 1 if OWN == 0 else 0


def trig_tables(blocks, rows, rope):
    half = rope // 2
    freq = 1.0 / ROPE_BASE ** (np.arange(half, dtype=np.float64) * 2.0 / rope)
    freq = np.concatenate([freq, freq])
    first = np.arange(blocks + 8, dtype=np.float64)[:, None] * rows * freq
    offset = np.arange(rows, dtype=np.float64)[:, None] * freq

    def both(angle):
        return np.concatenate([np.cos(angle), np.sin(angle)], axis=1).astype(np.float32)

    return np.concatenate([both(first), both(offset)], axis=0)


def half_swap(v):
    half = v.shape[-1] // 2
    return jnp.concatenate([v[..., half:], v[..., :half]], axis=-1)


def iota(shape, dim):
    return lax.broadcasted_iota(jnp.int32, shape, dim)


def sp_at(sp, dz, dy):
    return lax.rem(sp // 4 + dz, 4) * 4 + lax.rem(lax.rem(sp, 4) + dy, 4)


def lanes_of(sp, n):
    dz, dy = STEPS[n]
    return pl.ds(pl.multiple_of(256 * sp_at(sp, (4 - dz) % 4, (4 - dy) % 4), 256), 256)


def arranged(source):
    blocks = [source[t].astype(F32) for t in range(8)]
    lane = jnp.right_shift(iota((72, 128), 1), 5)
    for a in range(4):
        mine = [jnp.bitwise_and(lane - a, 3) == j for j in range(3)]
        halves = []
        for u in range(2):
            b = blocks[4 * u : 4 * u + 4]
            v = jnp.where(mine[0], b[0], jnp.where(mine[1], b[1], jnp.where(mine[2], b[2], b[3])))
            halves.append(pltpu.roll(v, 128 - 32 * a, 1) if a else v)
        both = jnp.concatenate(halves, axis=1)
        yield a, both[:64].astype(BF16), both[64:].astype(BF16)


def kernel(
    x_hbm, gain_hbm, w_hbm, rd_hbm, scal_hbm, look_hbm, pay_hbm, qn_hbm, qr_hbm, tab_hbm,
    stage, turned_stage, read_out,
    xb, gain, w, rd, scal, look, pay, tab,
    kst, kall, qn, qr, aall, pst, pall, ktst, krecv, asc, arecv, part, held,
    xsem, wsem, krsem, qrsem, small, k2rsem,
):
    sp, tp = lax.axis_index("sp"), lax.axis_index("tp")

    def tp_of(step):
        return lax.rem(tp + step, 8)

    ksend, k2send, psend, asend, csend = (wsem.at[n] for n in (1, 2, 4, 5, 6))
    qsend = (wsem.at[3], wsem.at[7])

    barrier = pltpu.get_barrier_semaphore()
    steps = sorted(STEPS, key=lambda s: -min(s[0], 4 - s[0]) - min(s[1], 4 - s[1]))[:15]

    def greet(some):
        for dz, dy in some:
            pl.semaphore_signal(barrier, inc=1, device_id=(sp_at(sp, dz, dy), tp), device_id_type=MESH)

    greet(steps[:5])

    halves = [pl.ds(0, 1024), pl.ds(1024, 1024)]
    loads = [
        pltpu.make_async_copy(src, dst, wsem.at[n % 9])
        for n, (src, dst) in enumerate(
            (
                (gain_hbm, gain), (w_hbm.at[halves[0]], w.at[halves[0], pl.ds(0, 512)]),
                (w_hbm.at[halves[1]], w.at[halves[1], pl.ds(0, 512)]),
                (rd_hbm, rd), (scal_hbm, scal), (tab_hbm, tab),
                (pay_hbm, pay), (qn_hbm, qn.at[tp]), (qr_hbm, qr.at[tp]), (look_hbm, look),
            )
        )
    ]
    for n in (6, 5, 0, 7, 8, 3):
        loads[n].start()
    for n in range(4):
        pltpu.make_async_copy(x_hbm.at[sp_at(sp, *STEPS[n])], xb.at[n], xsem.at[0]).start()
    loads[1].start()

    greet(steps[5:])
    for step in (4, 5, 3, 2, 6, 7, 1):
        pl.semaphore_signal(barrier, inc=1, device_id=(sp, tp_of(step)), device_id_type=MESH)
    for n in (4, 2):
        loads[n].start()

    def to_tp(src, dst, send, recv, step):
        return pltpu.make_async_remote_copy(
            src_ref=src, dst_ref=dst, send_sem=send, recv_sem=recv,
            device_id=(sp, tp_of(step)), device_id_type=MESH,
        )

    def to_all_tp(copies):
        for step in (4, 5, 3, 2, 6, 7, 1):
            for c in copies(step):
                c.start()

    def to_sp(src, dst, send, recv, n):
        return pltpu.make_async_remote_copy(
            src_ref=src, dst_ref=dst, send_sem=send, recv_sem=recv,
            device_id=(sp_at(sp, *STEPS[n]), tp), device_id_type=MESH,
        )

    row, col = iota((256, 256), 0), iota((256, 256), 1)
    wanted = jnp.bitwise_and(row, 15) * 16 + jnp.right_shift(row, 4)
    order = jnp.where(col == wanted, 1.0, 0.0).astype(BF16)
    loads[6].wait()
    for g in range(4):
        rows = jnp.dot(order, pay[256 * g : 256 * (g + 1), :], preferred_element_type=F32)
        rows = rows.astype(BF16).reshape(8, 2, 16, 128)
        for head in range(2):
            pst[:, 16 * g : 16 * (g + 1), 128 * head : 128 * (head + 1)] = rows[:, head]
    mine = pl.ds(pl.multiple_of(tp * 64, 64), 64)
    pall[mine, :] = pst[tp]

    loads[5].wait()
    sign = jnp.where(iota((32, 64), 1) < 32, -1.0, 1.0).astype(F32)
    base = tab[pl.ds(sp * 8 + tp, 1), :]
    offs = tab[136:]
    cos = base[:, :64] * offs[:, :64] - base[:, 64:] * offs[:, 64:]
    sin = (base[:, 64:] * offs[:, :64] + base[:, :64] * offs[:, 64:]) * sign
    loads[0].wait()

    loads[3].wait()
    w[:, 512:] = jnp.concatenate([rd[...].T, jnp.zeros((2048, 64), BF16)], axis=1)

    def project(k, groups):
        count = 4 * groups
        for n in range(groups):
            at = pl.ds(4 * (k + n), 4)
            pltpu.make_async_copy(x_hbm.at[pl.ds(0, 4)], xb.at[at], xsem.at[(k + n) % 2]).wait()
        if k == 1:
            for n in range(12, 16):
                pltpu.make_async_copy(x_hbm.at[sp_at(sp, *STEPS[n])], xb.at[n], xsem.at[n // 4 % 2]).start()
        xv = xb[4 * k : 4 * k + count].reshape(32 * count, 2048).astype(F32)
        scale = lax.rsqrt(jnp.mean(xv * xv, axis=1, keepdims=True) + EPS)
        normed = (xv * scale * gain[...]).astype(BF16)
        if k == 0:
            rot = jnp.dot(normed, w[:, 512:], preferred_element_type=F32)
        else:
            both = jnp.dot(normed, w[...], preferred_element_type=F32)
            latent, rot = both[:, :512], both[:, 512:]
        rot = rot[:, :64].astype(BF16).astype(F32)
        turn = [jnp.concatenate([part] * count, axis=0) for part in (cos, sin)]
        turned = (rot * turn[0] + half_swap(rot) * turn[1]).reshape(count, 2, 16, 64)
        turned = jnp.concatenate([turned[:, 0], turned[:, 1]], axis=-1).astype(BF16)
        kst[4 * k : 4 * k + count, 128:] = turned
        if k == 0:
            loads[1].wait()
            for n in range(4, 8):
                pltpu.make_async_copy(x_hbm.at[sp_at(sp, *STEPS[n])], xb.at[n], xsem.at[n // 4 % 2]).start()
            part[...] = jnp.dot(normed[:, :1024], w[:1024, :512], preferred_element_type=F32)
            held[...] = normed

            @pl.when(sp >= 0)
            def _():
                for n in (2, 4):
                    loads[n].wait()
                loads[9].start()
                for n in range(8, 12):
                    pltpu.make_async_copy(x_hbm.at[sp_at(sp, *STEPS[n])], xb.at[n], xsem.at[n // 4 % 2]).start()

            normed = held[...]
            latent = part[...] + jnp.dot(normed[:, 1024:], w[1024:, :512], preferred_element_type=F32)
        latent = latent.astype(BF16).astype(F32)
        scale = lax.rsqrt(jnp.mean(latent * latent, axis=1, keepdims=True) + EPS)
        stored = (latent * scale * scal[...]).astype(BF16).reshape(count, 32, 512)
        for b in range(4):
            kst[4 * k : 4 * k + count, 32 * b : 32 * b + 32] = stored[:, :, 128 * b : 128 * b + 128]
        if 4 * k <= OWN < 4 * k + count:
            slot = OWN // 4 * 4 + lax.rem(OWN + tp, 4)
            kall[slot] = kst[OWN]
        if k == 0:
            pl.semaphore_wait(barrier, 22)
        for n in range(4 * k, 4 * k + count):
            if n != OWN:
                slot = n // 4 * 4 + lax.rem(n + tp, 4)
                to_sp(kst.at[n], kall.at[slot], ksend, krsem.at[n // 4], n).start()

    def arrived(k):
        count = 4 if k != OWN // 4 else 3
        at = pl.ds(4 * k, count)
        to_sp(kst.at[at], kall.at[at], ksend, krsem.at[k], OTHERS).wait_recv()

    for n in (7, 8):
        loads[n].wait()
    project(0, 1)
    to_all_tp(
        lambda step: (
            to_tp(qn.at[tp], qn.at[tp], qsend[0], qrsem.at[0], step),
            to_tp(qr.at[tp], qr.at[tp], qsend[1], qrsem.at[1], step),
        )
    )
    to_all_tp(lambda step: (to_tp(pst.at[tp_of(step)], pall.at[mine, :], psend, small.at[0], step),))
    project(1, 1)

    project(2, 1)
    project(3, 1)

    loads[9].wait()
    seven = pl.ds(0, 7)
    to_tp(qn.at[seven], qn.at[seven], qsend[0], qrsem.at[0], 1).wait_recv()
    to_tp(qr.at[seven], qr.at[seven], qsend[1], qrsem.at[1], 1).wait_recv()
    q_all = qn[...].astype(F32).reshape(16, 128).astype(BF16)
    t_all = qr[...].astype(F32).reshape(16, 64)
    parts = lax.dot_general(q_all, look[...], NT, preferred_element_type=F32)
    same = jnp.bitwise_and(iota((16, 1024), 1), 15) == iota((16, 1024), 0)
    parts = jnp.where(same, parts, 0.0).astype(BF16)
    pick = jnp.right_shift(iota((1024, 128), 0), 4) + 64 * lax.rem(tp, 2) == iota((1024, 128), 1)
    pick = jnp.where(pick, 1.0, 0.0).astype(BF16)
    aall[tp] = jnp.dot(parts, pick, preferred_element_type=F32).astype(BF16)
    to_all_tp(lambda step: (to_tp(aall.at[tp], aall.at[tp], asend, small.at[1], step),))
    last = tab[128:129, :]
    q_turn = (t_all * last[:, :64] + half_swap(t_all) * (last[:, 64:] * sign[:1])).astype(BF16)

    def keys(k):
        packed = kall[4 * k : 4 * k + 4, 128:].astype(F32)
        swapped = half_swap(packed)
        rows = jnp.concatenate([packed[:, None, :, :64], swapped[:, None, :, :64]], axis=1)
        return rows.reshape(128, 64)

    def latents(k):
        return jnp.concatenate(
            [kall[4 * k : 4 * k + 4, 32 * b : 32 * b + 32].reshape(128, 128) for b in range(4)], axis=1
        )

    def turned_over(k):
        block, turned = latents(k).T, keys(k).T.astype(BF16)
        ktst[k, :, :64] = block.reshape(8, 64, 128)
        ktst[k, :, 64:] = turned.reshape(8, 8, 128)
        return block, turned

    def spread(k):
        to_all_tp(lambda step: (to_tp(ktst.at[k, tp_of(step)], krecv.at[k, tp], k2send, k2rsem.at[k], step),))
        krecv[k, tp] = ktst[k, tp]

    here = []
    for k in range(3):
        arrived(k)
        here.append(turned_over(k))
        spread(k)

    to_tp(aall.at[seven], aall.at[seven], asend, small.at[1], 1).wait_recv()
    absorbed = jnp.concatenate([aall[2 * u] + aall[2 * u + 1] for u in range(4)], axis=1)

    def scores(block, turned):
        total = jnp.dot(absorbed, block, preferred_element_type=F32)
        total += jnp.dot(q_turn, turned, preferred_element_type=F32)
        return total * (192.0 ** -0.5)

    def mixed(weight, k):
        return jnp.dot(weight.astype(BF16), latents(k), preferred_element_type=F32)

    seen = [scores(*group) for group in here]
    top_seen = jnp.max(jnp.maximum(jnp.maximum(seen[0], seen[1]), seen[2]), axis=1, keepdims=True)
    weights = [jnp.exp(s - top_seen) for s in seen]
    total_seen = jnp.sum(weights[0] + weights[1] + weights[2], axis=1, keepdims=True)
    context_seen = mixed(weights[0], 0) + mixed(weights[1], 1) + mixed(weights[2], 2)

    arrived(3)
    late = scores(*turned_over(3))
    top = jnp.maximum(top_seen, jnp.max(late, axis=1, keepdims=True))
    weight = jnp.exp(late - top)
    shrink = jnp.exp(top_seen - top)
    total = total_seen * shrink + jnp.sum(weight, axis=1, keepdims=True)
    context = context_seen * shrink + mixed(weight, 3)
    stats = jnp.where(iota((16, 128), 1) < 64, top, total)
    for t in range(8):
        asc[t, :, :512] = context[2 * t : 2 * t + 2]
        asc[t, :, 512:] = stats[2 * t : 2 * t + 2]
    to_all_tp(lambda step: (to_tp(asc.at[tp_of(step)], arecv.at[tp], csend, small.at[2], step),))
    arecv[tp] = asc[tp]
    spread(3)

    def arrange(k):
        to_tp(ktst.at[k, seven], krecv.at[k, seven], k2send, k2rsem.at[k], 1).wait_recv()
        for a, block, turned in arranged(krecv.at[k]):
            lanes = lanes_of(sp, 4 * k + a)
            stage[:, lanes] = block
            turned_stage[:, lanes] = turned

    for k in range(3):
        arrange(k)

    to_tp(pst.at[seven], pst.at[seven], psend, small.at[0], 1).wait_recv()
    to_tp(asc.at[seven], arecv.at[seven], csend, small.at[2], 1).wait_recv()
    got = arecv[...]
    tops, totals = got[:, :, 512:513], got[:, :, 576:577]
    share = jnp.exp(tops - jnp.max(tops, axis=0, keepdims=True))
    summed = jnp.sum(got[:, :, :512] * share, axis=0) / jnp.sum(totals * share, axis=0)
    summed = jnp.concatenate([summed, jnp.zeros((14, 512), F32)], axis=0).astype(BF16)
    values = jnp.dot(summed, pall[...], preferred_element_type=F32)
    values = jnp.where(iota((16, 128), 0) == 0, values[:, :128], values[:, 128:])[:2]
    values = values * lax.rsqrt(jnp.mean(values * values, axis=1, keepdims=True) + EPS)
    read_out[...] = values.astype(BF16)

    sent = pl.ds(OTHERS, 15)
    to_sp(kst.at[sent], kall.at[sent], ksend, krsem.at[0], OTHERS).wait_send()
    to_tp(qn.at[seven], qn.at[seven], qsend[0], qrsem.at[0], 1).wait_send()
    to_tp(qr.at[seven], qr.at[seven], qsend[1], qrsem.at[1], 1).wait_send()
    to_tp(pst.at[seven], pst.at[seven], psend, small.at[0], 1).wait_send()
    to_tp(aall.at[seven], aall.at[seven], asend, small.at[1], 1).wait_send()
    to_tp(asc.at[seven], arecv.at[seven], csend, small.at[2], 1).wait_send()
    to_tp(ktst.at[:, seven], ktst.at[:, seven], k2send, k2rsem.at[3], 1).wait_send()
    arrange(3)


def finish(stage, turned_stage, read_in, out_s, out_r, out_f, sem):
    pieces = 4
    for n in range(pieces):
        lanes = pl.ds(4096 // pieces * n, 4096 // pieces)
        pltpu.make_async_copy(stage.at[:, lanes], out_s.at[:, lanes], sem.at[0]).start()
    others = [
        pltpu.make_async_copy(turned_stage, out_r, sem.at[1]), pltpu.make_async_copy(read_in, out_f, sem.at[2])
    ]
    for c in others:
        c.start()
    pltpu.make_async_copy(stage, out_s, sem.at[0]).wait()
    for c in others:
        c.wait()


def solution(mesh):
    angles = trig_tables(128, 32, 64)

    def step(x, gain, w, rd, scal, look, payload, qn, qr):
        hbm = pl.BlockSpec(memory_space=pltpu.HBM)
        vmem = pl.BlockSpec(memory_space=pltpu.VMEM)
        dma = pltpu.SemaphoreType.DMA
        received = pl.pallas_call(
            kernel,
            out_shape=(
                jax.ShapeDtypeStruct((64, 4096), BF16),
                jax.ShapeDtypeStruct((8, 4096), BF16),
                jax.ShapeDtypeStruct((2, 128), BF16),
            ),
            in_specs=[hbm] * 10,
            out_specs=(vmem,) * 3,
            scratch_shapes=[
                pltpu.VMEM((16, 32, 2048), BF16),
                pltpu.VMEM((1, 2048), F32),
                pltpu.VMEM((2048, 640), BF16),
                pltpu.VMEM((64, 2048), BF16),
                pltpu.VMEM((1, 512), F32),
                pltpu.VMEM((1024, 128), BF16),
                pltpu.VMEM((1024, 128), BF16),
                pltpu.VMEM((168, 128), F32),
                pltpu.VMEM((16, 144, 128), BF16),
                pltpu.VMEM((16, 144, 128), BF16),
                pltpu.VMEM((8, 2, 128), BF16),
                pltpu.VMEM((8, 2, 64), BF16),
                pltpu.VMEM((8, 16, 128), BF16),
                pltpu.VMEM((8, 64, 256), BF16),
                pltpu.VMEM((512, 256), BF16),
                pltpu.VMEM((4, 8, 72, 128), BF16),
                pltpu.VMEM((4, 8, 72, 128), BF16),
                pltpu.VMEM((8, 2, 640), F32),
                pltpu.VMEM((8, 2, 640), F32),
                pltpu.VMEM((128, 512), F32),
                pltpu.VMEM((128, 2048), BF16),
                dma((2,)),
                dma((9,)),
                dma((4,)),
                dma((2,)),
                dma((3,)),
                dma((4,)),
            ],
            compiler_params=pltpu.CompilerParams(
                collective_id=0, has_side_effects=True, vmem_limit_bytes=48 * 1024 * 1024
            ),
        )(
            *(
                pltpu.with_memory_space_constraint(v, pltpu.HBM)
                for v in (
                    x, gain.reshape(1, 2048), w, rd.T, scal.reshape(1, 512), look.reshape(1024, 128),
                    payload.reshape(1024, 128), qn.reshape(2, 128), qr.reshape(2, 64),
                    jnp.asarray(angles),
                )
            )
        )
        stored, rotary, read = pl.pallas_call(
            finish,
            out_shape=(
                jax.ShapeDtypeStruct((64, 4096), BF16),
                jax.ShapeDtypeStruct((8, 4096), BF16),
                jax.ShapeDtypeStruct((2, 128), BF16),
            ),
            in_specs=[vmem] * 3,
            out_specs=(hbm,) * 3,
            scratch_shapes=[dma((3,))],
        )(*(pltpu.with_memory_space_constraint(v, pltpu.VMEM) for v in received))
        return stored.T[None], rotary.T[None], read[None]

    tp = "tp"
    both = ("sp", "tp")
    in_specs = (
        P(None, both, None), P(), P(), P(), P(), P(tp, None, None), P(tp, None, None),
        P("sp", tp, None), P("sp", tp, None),
    )
    out_specs = (P("sp", None, tp), P("sp", None, tp), P("sp", tp, None))
    return jax.shard_map(step, mesh=mesh, in_specs=in_specs, out_specs=out_specs, check_vma=False)
```

```python
import jax
import jax.numpy as jnp
import numpy as np
from jax import lax
from jax.experimental import pallas as pl
from jax.experimental.pallas import tpu as pltpu
from jax.sharding import PartitionSpec as P

MESH = pl.DeviceIdType.MESH
EPS = 1e-6
ROPE_BASE = 10000.0
F32 = jnp.float32
BF16 = jnp.bfloat16

NT = (((1,), (1,)), ((), ()))

STEPS = (
    (2, 0), (0, 2), (1, 1), (3, 3),
    (1, 2), (3, 2), (1, 3), (3, 1),
    (2, 1), (2, 3), (1, 0), (3, 0),
    (2, 2), (0, 1), (0, 3), (0, 0),
)
OWN = STEPS.index((0, 0))
OTHERS = 1 if OWN == 0 else 0


def trig_tables(blocks, rows, rope):
    half = rope // 2
    freq = 1.0 / ROPE_BASE ** (np.arange(half, dtype=np.float64) * 2.0 / rope)
    freq = np.concatenate([freq, freq])
    first = np.arange(blocks + 8, dtype=np.float64)[:, None] * rows * freq
    offset = np.arange(rows, dtype=np.float64)[:, None] * freq

    def both(angle):
        return np.concatenate([np.cos(angle), np.sin(angle)], axis=1).astype(np.float32)

    return np.concatenate([both(first), both(offset)], axis=0)


def half_swap(v):
    half = v.shape[-1] // 2
    return jnp.concatenate([v[..., half:], v[..., :half]], axis=-1)


def iota(shape, dim):
    return lax.broadcasted_iota(jnp.int32, shape, dim)


def sp_at(sp, dz, dy):
    return lax.rem(sp // 4 + dz, 4) * 4 + lax.rem(lax.rem(sp, 4) + dy, 4)


def lanes_of(sp, n):
    dz, dy = STEPS[n]
    return pl.ds(pl.multiple_of(256 * sp_at(sp, (4 - dz) % 4, (4 - dy) % 4), 256), 256)


def arranged(source):
    blocks = [source[t].astype(F32) for t in range(8)]
    lane = jnp.right_shift(iota((72, 128), 1), 5)
    for a in range(4):
        mine = [jnp.bitwise_and(lane - a, 3) == j for j in range(3)]
        halves = []
        for u in range(2):
            b = blocks[4 * u : 4 * u + 4]
            v = jnp.where(mine[0], b[0], jnp.where(mine[1], b[1], jnp.where(mine[2], b[2], b[3])))
            halves.append(pltpu.roll(v, 128 - 32 * a, 1) if a else v)
        both = jnp.concatenate(halves, axis=1)
        yield a, both[:64].astype(BF16), both[64:].astype(BF16)


def kernel(
    x_hbm, gain_hbm, w_hbm, rd_hbm, scal_hbm, look_hbm, pay_hbm, qn_hbm, qr_hbm, tab_hbm,
    stage, turned_stage, read_out,
    xb, gain, w, rd, scal, look, pay, tab,
    kst, kall, qn, qr, aall, pst, pall, ktst, krecv, asc, arecv, part, held,
    xsem, wsem, krsem, qrsem, small, k2rsem,
):
    sp, tp = lax.axis_index("sp"), lax.axis_index("tp")

    def tp_of(step):
        return lax.rem(tp + step, 8)

    ksend, k2send, psend, asend, csend = (wsem.at[n] for n in (1, 2, 4, 5, 6))
    qsend = (wsem.at[3], wsem.at[7])

    barrier = pltpu.get_barrier_semaphore()
    steps = sorted(STEPS, key=lambda s: -min(s[0], 4 - s[0]) - min(s[1], 4 - s[1]))[:15]

    def greet(some):
        for dz, dy in some:
            pl.semaphore_signal(barrier, inc=1, device_id=(sp_at(sp, dz, dy), tp), device_id_type=MESH)

    greet(steps[:5])

    halves = [pl.ds(0, 1024), pl.ds(1024, 1024)]
    loads = [
        pltpu.make_async_copy(src, dst, wsem.at[n % 9])
        for n, (src, dst) in enumerate(
            (
                (gain_hbm, gain), (w_hbm.at[halves[0]], w.at[halves[0], pl.ds(0, 512)]),
                (w_hbm.at[halves[1]], w.at[halves[1], pl.ds(0, 512)]),
                (rd_hbm, rd), (scal_hbm, scal), (tab_hbm, tab),
                (pay_hbm, pay), (qn_hbm, qn.at[tp]), (qr_hbm, qr.at[tp]), (look_hbm, look),
            )
        )
    ]
    for n in (6, 5, 0, 7, 8, 3):
        loads[n].start()
    for n in range(4):
        pltpu.make_async_copy(x_hbm.at[sp_at(sp, *STEPS[n])], xb.at[n], xsem.at[0]).start()
    loads[1].start()

    greet(steps[5:])
    for step in (4, 5, 3, 2, 6, 7, 1):
        pl.semaphore_signal(barrier, inc=1, device_id=(sp, tp_of(step)), device_id_type=MESH)
    for n in (4, 2):
        loads[n].start()

    def to_tp(src, dst, send, recv, step):
        return pltpu.make_async_remote_copy(
            src_ref=src, dst_ref=dst, send_sem=send, recv_sem=recv,
            device_id=(sp, tp_of(step)), device_id_type=MESH,
        )

    def to_all_tp(copies):
        for step in (4, 5, 3, 2, 6, 7, 1):
            for c in copies(step):
                c.start()

    def to_sp(src, dst, send, recv, n):
        return pltpu.make_async_remote_copy(
            src_ref=src, dst_ref=dst, send_sem=send, recv_sem=recv,
            device_id=(sp_at(sp, *STEPS[n]), tp), device_id_type=MESH,
        )

    row, col = iota((256, 256), 0), iota((256, 256), 1)
    wanted = jnp.bitwise_and(row, 15) * 16 + jnp.right_shift(row, 4)
    order = jnp.where(col == wanted, 1.0, 0.0).astype(BF16)
    loads[6].wait()
    for g in range(4):
        rows = jnp.dot(order, pay[256 * g : 256 * (g + 1), :], preferred_element_type=F32)
        rows = rows.astype(BF16).reshape(8, 2, 16, 128)
        for head in range(2):
            pst[:, 16 * g : 16 * (g + 1), 128 * head : 128 * (head + 1)] = rows[:, head]
    mine = pl.ds(pl.multiple_of(tp * 64, 64), 64)
    pall[mine, :] = pst[tp]

    loads[5].wait()
    sign = jnp.where(iota((32, 64), 1) < 32, -1.0, 1.0).astype(F32)
    base = tab[pl.ds(sp * 8 + tp, 1), :]
    offs = tab[136:]
    cos = base[:, :64] * offs[:, :64] - base[:, 64:] * offs[:, 64:]
    sin = (base[:, 64:] * offs[:, :64] + base[:, :64] * offs[:, 64:]) * sign
    loads[0].wait()

    loads[3].wait()
    w[:, 512:] = jnp.concatenate([rd[...].T, jnp.zeros((2048, 64), BF16)], axis=1)

    def project(k, groups):
        count = 4 * groups
        for n in range(groups):
            at = pl.ds(4 * (k + n), 4)
            pltpu.make_async_copy(x_hbm.at[pl.ds(0, 4)], xb.at[at], xsem.at[(k + n) % 2]).wait()
        if k == 1:
            for n in range(12, 16):
                pltpu.make_async_copy(x_hbm.at[sp_at(sp, *STEPS[n])], xb.at[n], xsem.at[n // 4 % 2]).start()
        xv = xb[4 * k : 4 * k + count].reshape(32 * count, 2048).astype(F32)
        scale = lax.rsqrt(jnp.mean(xv * xv, axis=1, keepdims=True) + EPS)
        normed = (xv * scale * gain[...]).astype(BF16)
        if k == 0:
            rot = jnp.dot(normed, w[:, 512:], preferred_element_type=F32)
        else:
            both = jnp.dot(normed, w[...], preferred_element_type=F32)
            latent, rot = both[:, :512], both[:, 512:]
        rot = rot[:, :64].astype(BF16).astype(F32)
        turn = [jnp.concatenate([part] * count, axis=0) for part in (cos, sin)]
        turned = (rot * turn[0] + half_swap(rot) * turn[1]).reshape(count, 2, 16, 64)
        turned = jnp.concatenate([turned[:, 0], turned[:, 1]], axis=-1).astype(BF16)
        kst[4 * k : 4 * k + count, 128:] = turned
        if k == 0:
            loads[1].wait()
            for n in range(4, 8):
                pltpu.make_async_copy(x_hbm.at[sp_at(sp, *STEPS[n])], xb.at[n], xsem.at[n // 4 % 2]).start()
            part[...] = jnp.dot(normed[:, :1024], w[:1024, :512], preferred_element_type=F32)
            held[...] = normed

            @pl.when(sp >= 0)
            def _():
                for n in (2, 4):
                    loads[n].wait()
                loads[9].start()
                for n in range(8, 12):
                    pltpu.make_async_copy(x_hbm.at[sp_at(sp, *STEPS[n])], xb.at[n], xsem.at[n // 4 % 2]).start()

            normed = held[...]
            latent = part[...] + jnp.dot(normed[:, 1024:], w[1024:, :512], preferred_element_type=F32)
        latent = latent.astype(BF16).astype(F32)
        scale = lax.rsqrt(jnp.mean(latent * latent, axis=1, keepdims=True) + EPS)
        stored = (latent * scale * scal[...]).astype(BF16).reshape(count, 32, 512)
        for b in range(4):
            kst[4 * k : 4 * k + count, 32 * b : 32 * b + 32] = stored[:, :, 128 * b : 128 * b + 128]
        if 4 * k <= OWN < 4 * k + count:
            slot = OWN // 4 * 4 + lax.rem(OWN + tp, 4)
            kall[slot] = kst[OWN]
        if k == 0:
            pl.semaphore_wait(barrier, 22)
        for n in range(4 * k, 4 * k + count):
            if n != OWN:
                slot = n // 4 * 4 + lax.rem(n + tp, 4)
                to_sp(kst.at[n], kall.at[slot], ksend, krsem.at[n // 4], n).start()

    def arrived(k):
        count = 4 if k != OWN // 4 else 3
        at = pl.ds(4 * k, count)
        to_sp(kst.at[at], kall.at[at], ksend, krsem.at[k], OTHERS).wait_recv()

    for n in (7, 8):
        loads[n].wait()
    project(0, 1)
    to_all_tp(
        lambda step: (
            to_tp(qn.at[tp], qn.at[tp], qsend[0], qrsem.at[0], step),
            to_tp(qr.at[tp], qr.at[tp], qsend[1], qrsem.at[1], step),
        )
    )
    to_all_tp(lambda step: (to_tp(pst.at[tp_of(step)], pall.at[mine, :], psend, small.at[0], step),))
    project(1, 1)

    project(2, 1)
    project(3, 1)

    loads[9].wait()
    seven = pl.ds(0, 7)
    to_tp(qn.at[seven], qn.at[seven], qsend[0], qrsem.at[0], 1).wait_recv()
    to_tp(qr.at[seven], qr.at[seven], qsend[1], qrsem.at[1], 1).wait_recv()
    q_all = qn[...].astype(F32).reshape(16, 128).astype(BF16)
    t_all = qr[...].astype(F32).reshape(16, 64)
    parts = lax.dot_general(q_all, look[...], NT, preferred_element_type=F32)
    same = jnp.bitwise_and(iota((16, 1024), 1), 15) == iota((16, 1024), 0)
    parts = jnp.where(same, parts, 0.0).astype(BF16)
    pick = jnp.right_shift(iota((1024, 128), 0), 4) + 64 * lax.rem(tp, 2) == iota((1024, 128), 1)
    pick = jnp.where(pick, 1.0, 0.0).astype(BF16)
    aall[tp] = jnp.dot(parts, pick, preferred_element_type=F32).astype(BF16)
    to_all_tp(lambda step: (to_tp(aall.at[tp], aall.at[tp], asend, small.at[1], step),))
    last = tab[128:129, :]
    q_turn = (t_all * last[:, :64] + half_swap(t_all) * (last[:, 64:] * sign[:1])).astype(BF16)

    def keys(k):
        packed = kall[4 * k : 4 * k + 4, 128:].astype(F32)
        swapped = half_swap(packed)
        rows = jnp.concatenate([packed[:, None, :, :64], swapped[:, None, :, :64]], axis=1)
        return rows.reshape(128, 64)

    def latents(k):
        return jnp.concatenate(
            [kall[4 * k : 4 * k + 4, 32 * b : 32 * b + 32].reshape(128, 128) for b in range(4)], axis=1
        )

    def turned_over(k):
        block, turned = latents(k).T, keys(k).T.astype(BF16)
        ktst[k, :, :64] = block.reshape(8, 64, 128)
        ktst[k, :, 64:] = turned.reshape(8, 8, 128)
        return block, turned

    def spread(k):
        to_all_tp(lambda step: (to_tp(ktst.at[k, tp_of(step)], krecv.at[k, tp], k2send, k2rsem.at[k], step),))
        krecv[k, tp] = ktst[k, tp]

    here = []
    for k in range(3):
        arrived(k)
        here.append(turned_over(k))
        spread(k)

    to_tp(aall.at[seven], aall.at[seven], asend, small.at[1], 1).wait_recv()
    absorbed = jnp.concatenate([aall[2 * u] + aall[2 * u + 1] for u in range(4)], axis=1)

    def scores(block, turned):
        total = jnp.dot(absorbed, block, preferred_element_type=F32)
        total += jnp.dot(q_turn, turned, preferred_element_type=F32)
        return total * (192.0 ** -0.5)

    def mixed(weight, k):
        return jnp.dot(weight.astype(BF16), latents(k), preferred_element_type=F32)

    seen = [scores(*group) for group in here]
    top_seen = jnp.max(jnp.maximum(jnp.maximum(seen[0], seen[1]), seen[2]), axis=1, keepdims=True)
    weights = [jnp.exp(s - top_seen) for s in seen]
    total_seen = jnp.sum(weights[0] + weights[1] + weights[2], axis=1, keepdims=True)
    context_seen = mixed(weights[0], 0) + mixed(weights[1], 1) + mixed(weights[2], 2)

    arrived(3)
    late = scores(*turned_over(3))
    top = jnp.maximum(top_seen, jnp.max(late, axis=1, keepdims=True))
    weight = jnp.exp(late - top)
    shrink = jnp.exp(top_seen - top)
    total = total_seen * shrink + jnp.sum(weight, axis=1, keepdims=True)
    context = context_seen * shrink + mixed(weight, 3)
    stats = jnp.where(iota((16, 128), 1) < 64, top, total)
    for t in range(8):
        asc[t, :, :512] = context[2 * t : 2 * t + 2]
        asc[t, :, 512:] = stats[2 * t : 2 * t + 2]
    to_all_tp(lambda step: (to_tp(asc.at[tp_of(step)], arecv.at[tp], csend, small.at[2], step),))
    arecv[tp] = asc[tp]
    spread(3)

    def arrange(k):
        to_tp(ktst.at[k, seven], krecv.at[k, seven], k2send, k2rsem.at[k], 1).wait_recv()
        for a, block, turned in arranged(krecv.at[k]):
            lanes = lanes_of(sp, 4 * k + a)
            stage[:, lanes] = block
            turned_stage[:, lanes] = turned

    for k in range(3):
        arrange(k)

    to_tp(pst.at[seven], pst.at[seven], psend, small.at[0], 1).wait_recv()
    to_tp(asc.at[seven], arecv.at[seven], csend, small.at[2], 1).wait_recv()
    got = arecv[...]
    tops, totals = got[:, :, 512:513], got[:, :, 576:577]
    share = jnp.exp(tops - jnp.max(tops, axis=0, keepdims=True))
    summed = jnp.sum(got[:, :, :512] * share, axis=0) / jnp.sum(totals * share, axis=0)
    summed = jnp.concatenate([summed, jnp.zeros((14, 512), F32)], axis=0).astype(BF16)
    values = jnp.dot(summed, pall[...], preferred_element_type=F32)
    values = jnp.where(iota((16, 128), 0) == 0, values[:, :128], values[:, 128:])[:2]
    values = values * lax.rsqrt(jnp.mean(values * values, axis=1, keepdims=True) + EPS)
    read_out[...] = values.astype(BF16)

    sent = pl.ds(OTHERS, 15)
    to_sp(kst.at[sent], kall.at[sent], ksend, krsem.at[0], OTHERS).wait_send()
    to_tp(qn.at[seven], qn.at[seven], qsend[0], qrsem.at[0], 1).wait_send()
    to_tp(qr.at[seven], qr.at[seven], qsend[1], qrsem.at[1], 1).wait_send()
    to_tp(pst.at[seven], pst.at[seven], psend, small.at[0], 1).wait_send()
    to_tp(aall.at[seven], aall.at[seven], asend, small.at[1], 1).wait_send()
    to_tp(asc.at[seven], arecv.at[seven], csend, small.at[2], 1).wait_send()
    to_tp(ktst.at[:, seven], ktst.at[:, seven], k2send, k2rsem.at[3], 1).wait_send()
    arrange(3)


def finish(stage, turned_stage, read_in, out_s, out_r, out_f, sem):
    pieces = 4
    for n in range(pieces):
        lanes = pl.ds(4096 // pieces * n, 4096 // pieces)
        pltpu.make_async_copy(stage.at[:, lanes], out_s.at[:, lanes], sem.at[0]).start()
    others = [
        pltpu.make_async_copy(turned_stage, out_r, sem.at[1]), pltpu.make_async_copy(read_in, out_f, sem.at[2])
    ]
    for c in others:
        c.start()
    pltpu.make_async_copy(stage, out_s, sem.at[0]).wait()
    for c in others:
        c.wait()


def solution(mesh):
    angles = trig_tables(128, 32, 64)

    def step(x, gain, w, rd, scal, look, payload, qn, qr):
        hbm = pl.BlockSpec(memory_space=pltpu.HBM)
        vmem = pl.BlockSpec(memory_space=pltpu.VMEM)
        dma = pltpu.SemaphoreType.DMA
        received = pl.pallas_call(
            kernel,
            out_shape=(
                jax.ShapeDtypeStruct((64, 4096), BF16),
                jax.ShapeDtypeStruct((8, 4096), BF16),
                jax.ShapeDtypeStruct((2, 128), BF16),
            ),
            in_specs=[hbm] * 10,
            out_specs=(vmem,) * 3,
            scratch_shapes=[
                pltpu.VMEM((16, 32, 2048), BF16),
                pltpu.VMEM((1, 2048), F32),
                pltpu.VMEM((2048, 640), BF16),
                pltpu.VMEM((64, 2048), BF16),
                pltpu.VMEM((1, 512), F32),
                pltpu.VMEM((1024, 128), BF16),
                pltpu.VMEM((1024, 128), BF16),
                pltpu.VMEM((168, 128), F32),
                pltpu.VMEM((16, 144, 128), BF16),
                pltpu.VMEM((16, 144, 128), BF16),
                pltpu.VMEM((8, 2, 128), BF16),
                pltpu.VMEM((8, 2, 64), BF16),
                pltpu.VMEM((8, 16, 128), BF16),
                pltpu.VMEM((8, 64, 256), BF16),
                pltpu.VMEM((512, 256), BF16),
                pltpu.VMEM((4, 8, 72, 128), BF16),
                pltpu.VMEM((4, 8, 72, 128), BF16),
                pltpu.VMEM((8, 2, 640), F32),
                pltpu.VMEM((8, 2, 640), F32),
                pltpu.VMEM((128, 512), F32),
                pltpu.VMEM((128, 2048), BF16),
                dma((2,)),
                dma((9,)),
                dma((4,)),
                dma((2,)),
                dma((3,)),
                dma((4,)),
            ],
            compiler_params=pltpu.CompilerParams(
                collective_id=0, has_side_effects=True, vmem_limit_bytes=48 * 1024 * 1024
            ),
        )(
            *(
                pltpu.with_memory_space_constraint(v, pltpu.HBM)
                for v in (
                    x, gain.reshape(1, 2048), w, rd.T, scal.reshape(1, 512), look.reshape(1024, 128),
                    payload.reshape(1024, 128), qn.reshape(2, 128), qr.reshape(2, 64),
                    jnp.asarray(angles),
                )
            )
        )
        stored, rotary, read = pl.pallas_call(
            finish,
            out_shape=(
                jax.ShapeDtypeStruct((64, 4096), BF16),
                jax.ShapeDtypeStruct((8, 4096), BF16),
                jax.ShapeDtypeStruct((2, 128), BF16),
            ),
            in_specs=[vmem] * 3,
            out_specs=(hbm,) * 3,
            scratch_shapes=[dma((3,))],
        )(*(pltpu.with_memory_space_constraint(v, pltpu.VMEM) for v in received))
        return stored.T[None], rotary.T[None], read[None]

    tp = "tp"
    both = ("sp", "tp")
    in_specs = (
        P(None, both, None), P(), P(), P(), P(), P(tp, None, None), P(tp, None, None),
        P("sp", tp, None), P("sp", tp, None),
    )
    out_specs = (P("sp", None, tp), P("sp", None, tp), P("sp", tp, None))
    return jax.shard_map(step, mesh=mesh, in_specs=in_specs, out_specs=out_specs, check_vma=False)
```

```python
import jax
import jax.numpy as jnp
import numpy as np
from jax import lax
from jax.experimental import pallas as pl
from jax.experimental.pallas import tpu as pltpu
from jax.sharding import PartitionSpec as P

MESH = pl.DeviceIdType.MESH
EPS = 1e-6
ROPE_BASE = 10000.0
F32 = jnp.float32
BF16 = jnp.bfloat16

NT = (((1,), (1,)), ((), ()))

STEPS = (
    (2, 0), (0, 2), (1, 1), (3, 3),
    (1, 2), (3, 2), (1, 3), (3, 1),
    (2, 1), (2, 3), (1, 0), (3, 0),
    (2, 2), (0, 1), (0, 3), (0, 0),
)
OWN = STEPS.index((0, 0))
OTHERS = 1 if OWN == 0 else 0


def trig_tables(blocks, rows, rope):
    half = rope // 2
    freq = 1.0 / ROPE_BASE ** (np.arange(half, dtype=np.float64) * 2.0 / rope)
    freq = np.concatenate([freq, freq])
    first = np.arange(blocks + 8, dtype=np.float64)[:, None] * rows * freq
    offset = np.arange(rows, dtype=np.float64)[:, None] * freq

    def both(angle):
        return np.concatenate([np.cos(angle), np.sin(angle)], axis=1).astype(np.float32)

    return np.concatenate([both(first), both(offset)], axis=0)


def half_swap(v):
    half = v.shape[-1] // 2
    return jnp.concatenate([v[..., half:], v[..., :half]], axis=-1)


def iota(shape, dim):
    return lax.broadcasted_iota(jnp.int32, shape, dim)


def sp_at(sp, dz, dy):
    return lax.rem(sp // 4 + dz, 4) * 4 + lax.rem(lax.rem(sp, 4) + dy, 4)


def lanes_of(sp, n):
    dz, dy = STEPS[n]
    return pl.ds(pl.multiple_of(256 * sp_at(sp, (4 - dz) % 4, (4 - dy) % 4), 256), 256)


def arranged(source):
    blocks = [source[t].astype(F32) for t in range(8)]
    lane = jnp.right_shift(iota((72, 128), 1), 5)
    for a in range(4):
        mine = [jnp.bitwise_and(lane - a, 3) == j for j in range(3)]
        halves = []
        for u in range(2):
            b = blocks[4 * u : 4 * u + 4]
            v = jnp.where(mine[0], b[0], jnp.where(mine[1], b[1], jnp.where(mine[2], b[2], b[3])))
            halves.append(pltpu.roll(v, 128 - 32 * a, 1) if a else v)
        both = jnp.concatenate(halves, axis=1)
        yield a, both[:64].astype(BF16), both[64:].astype(BF16)


def kernel(
    x_hbm, gain_hbm, w_hbm, rd_hbm, scal_hbm, look_hbm, pay_hbm, qn_hbm, qr_hbm, tab_hbm,
    stage, turned_stage, read_out,
    xb, gain, w, rd, scal, look, pay, tab,
    kst, kall, qn, qr, aall, pst, pall, ktst, krecv, asc, arecv, part, held,
    xsem, wsem, krsem, qrsem, small, k2rsem,
):
    sp, tp = lax.axis_index("sp"), lax.axis_index("tp")

    def tp_of(step):
        return lax.rem(tp + step, 8)

    ksend, k2send, psend, asend, csend = (wsem.at[n] for n in (1, 2, 4, 5, 6))
    qsend = (wsem.at[3], wsem.at[7])

    barrier = pltpu.get_barrier_semaphore()
    steps = sorted(STEPS, key=lambda s: -min(s[0], 4 - s[0]) - min(s[1], 4 - s[1]))[:15]

    def greet(some):
        for dz, dy in some:
            pl.semaphore_signal(barrier, inc=1, device_id=(sp_at(sp, dz, dy), tp), device_id_type=MESH)

    greet(steps[:5])

    halves = [pl.ds(0, 1024), pl.ds(1024, 1024)]
    loads = [
        pltpu.make_async_copy(src, dst, wsem.at[n % 9])
        for n, (src, dst) in enumerate(
            (
                (gain_hbm, gain), (w_hbm.at[halves[0]], w.at[halves[0], pl.ds(0, 512)]),
                (w_hbm.at[halves[1]], w.at[halves[1], pl.ds(0, 512)]),
                (rd_hbm, rd), (scal_hbm, scal), (tab_hbm, tab),
                (pay_hbm, pay), (qn_hbm, qn.at[tp]), (qr_hbm, qr.at[tp]), (look_hbm, look),
            )
        )
    ]
    for n in (6, 5, 0, 7, 8, 3):
        loads[n].start()
    for n in range(4):
        pltpu.make_async_copy(x_hbm.at[sp_at(sp, *STEPS[n])], xb.at[n], xsem.at[0]).start()
    loads[1].start()

    greet(steps[5:])
    for step in (4, 5, 3, 2, 6, 7, 1):
        pl.semaphore_signal(barrier, inc=1, device_id=(sp, tp_of(step)), device_id_type=MESH)
    for n in (4, 2):
        loads[n].start()

    def to_tp(src, dst, send, recv, step):
        return pltpu.make_async_remote_copy(
            src_ref=src, dst_ref=dst, send_sem=send, recv_sem=recv,
            device_id=(sp, tp_of(step)), device_id_type=MESH,
        )

    def to_all_tp(copies):
        for step in (4, 5, 3, 2, 6, 7, 1):
            for c in copies(step):
                c.start()

    def to_sp(src, dst, send, recv, n):
        return pltpu.make_async_remote_copy(
            src_ref=src, dst_ref=dst, send_sem=send, recv_sem=recv,
            device_id=(sp_at(sp, *STEPS[n]), tp), device_id_type=MESH,
        )

    row, col = iota((256, 256), 0), iota((256, 256), 1)
    wanted = jnp.bitwise_and(row, 15) * 16 + jnp.right_shift(row, 4)
    order = jnp.where(col == wanted, 1.0, 0.0).astype(BF16)
    loads[6].wait()
    for g in range(4):
        rows = jnp.dot(order, pay[256 * g : 256 * (g + 1), :], preferred_element_type=F32)
        rows = rows.astype(BF16).reshape(8, 2, 16, 128)
        for head in range(2):
            pst[:, 16 * g : 16 * (g + 1), 128 * head : 128 * (head + 1)] = rows[:, head]
    mine = pl.ds(pl.multiple_of(tp * 64, 64), 64)
    pall[mine, :] = pst[tp]

    loads[5].wait()
    sign = jnp.where(iota((32, 64), 1) < 32, -1.0, 1.0).astype(F32)
    base = tab[pl.ds(sp * 8 + tp, 1), :]
    offs = tab[136:]
    cos = base[:, :64] * offs[:, :64] - base[:, 64:] * offs[:, 64:]
    sin = (base[:, 64:] * offs[:, :64] + base[:, :64] * offs[:, 64:]) * sign
    loads[0].wait()

    loads[3].wait()
    w[:, 512:] = jnp.concatenate([rd[...].T, jnp.zeros((2048, 64), BF16)], axis=1)

    def project(k, groups):
        count = 4 * groups
        for n in range(groups):
            at = pl.ds(4 * (k + n), 4)
            pltpu.make_async_copy(x_hbm.at[pl.ds(0, 4)], xb.at[at], xsem.at[(k + n) % 2]).wait()
        if k == 1:
            for n in range(12, 16):
                pltpu.make_async_copy(x_hbm.at[sp_at(sp, *STEPS[n])], xb.at[n], xsem.at[n // 4 % 2]).start()
        xv = xb[4 * k : 4 * k + count].reshape(32 * count, 2048).astype(F32)
        scale = lax.rsqrt(jnp.mean(xv * xv, axis=1, keepdims=True) + EPS)
        normed = (xv * scale * gain[...]).astype(BF16)
        if k == 0:
            rot = jnp.dot(normed, w[:, 512:], preferred_element_type=F32)
        else:
            both = jnp.dot(normed, w[...], preferred_element_type=F32)
            latent, rot = both[:, :512], both[:, 512:]
        rot = rot[:, :64].astype(BF16).astype(F32)
        turn = [jnp.concatenate([part] * count, axis=0) for part in (cos, sin)]
        turned = (rot * turn[0] + half_swap(rot) * turn[1]).reshape(count, 2, 16, 64)
        turned = jnp.concatenate([turned[:, 0], turned[:, 1]], axis=-1).astype(BF16)
        kst[4 * k : 4 * k + count, 128:] = turned
        if k == 0:
            loads[1].wait()
            for n in range(4, 8):
                pltpu.make_async_copy(x_hbm.at[sp_at(sp, *STEPS[n])], xb.at[n], xsem.at[n // 4 % 2]).start()
            part[...] = jnp.dot(normed[:, :1024], w[:1024, :512], preferred_element_type=F32)
            held[...] = normed

            @pl.when(sp >= 0)
            def _():
                for n in (2, 4):
                    loads[n].wait()
                loads[9].start()
                for n in range(8, 12):
                    pltpu.make_async_copy(x_hbm.at[sp_at(sp, *STEPS[n])], xb.at[n], xsem.at[n // 4 % 2]).start()

            normed = held[...]
            latent = part[...] + jnp.dot(normed[:, 1024:], w[1024:, :512], preferred_element_type=F32)
        latent = latent.astype(BF16).astype(F32)
        scale = lax.rsqrt(jnp.mean(latent * latent, axis=1, keepdims=True) + EPS)
        stored = (latent * scale * scal[...]).astype(BF16).reshape(count, 32, 512)
        for b in range(4):
            kst[4 * k : 4 * k + count, 32 * b : 32 * b + 32] = stored[:, :, 128 * b : 128 * b + 128]
        if 4 * k <= OWN < 4 * k + count:
            slot = OWN // 4 * 4 + lax.rem(OWN + tp, 4)
            kall[slot] = kst[OWN]
        if k == 0:
            pl.semaphore_wait(barrier, 22)
        for n in range(4 * k, 4 * k + count):
            if n != OWN:
                slot = n // 4 * 4 + lax.rem(n + tp, 4)
                to_sp(kst.at[n], kall.at[slot], ksend, krsem.at[n // 4], n).start()

    def arrived(k):
        count = 4 if k != OWN // 4 else 3
        at = pl.ds(4 * k, count)
        to_sp(kst.at[at], kall.at[at], ksend, krsem.at[k], OTHERS).wait_recv()

    for n in (7, 8):
        loads[n].wait()
    project(0, 1)
    to_all_tp(
        lambda step: (
            to_tp(qn.at[tp], qn.at[tp], qsend[0], qrsem.at[0], step),
            to_tp(qr.at[tp], qr.at[tp], qsend[1], qrsem.at[1], step),
        )
    )
    project(1, 1)
    to_all_tp(lambda step: (to_tp(pst.at[tp_of(step)], pall.at[mine, :], psend, small.at[0], step),))

    project(2, 1)
    project(3, 1)

    loads[9].wait()
    seven = pl.ds(0, 7)
    to_tp(qn.at[seven], qn.at[seven], qsend[0], qrsem.at[0], 1).wait_recv()
    to_tp(qr.at[seven], qr.at[seven], qsend[1], qrsem.at[1], 1).wait_recv()
    q_all = qn[...].astype(F32).reshape(16, 128).astype(BF16)
    t_all = qr[...].astype(F32).reshape(16, 64)
    parts = lax.dot_general(q_all, look[...], NT, preferred_element_type=F32)
    same = jnp.bitwise_and(iota((16, 1024), 1), 15) == iota((16, 1024), 0)
    parts = jnp.where(same, parts, 0.0).astype(BF16)
    pick = jnp.right_shift(iota((1024, 128), 0), 4) + 64 * lax.rem(tp, 2) == iota((1024, 128), 1)
    pick = jnp.where(pick, 1.0, 0.0).astype(BF16)
    aall[tp] = jnp.dot(parts, pick, preferred_element_type=F32).astype(BF16)
    to_all_tp(lambda step: (to_tp(aall.at[tp], aall.at[tp], asend, small.at[1], step),))
    last = tab[128:129, :]
    q_turn = (t_all * last[:, :64] + half_swap(t_all) * (last[:, 64:] * sign[:1])).astype(BF16)

    def keys(k):
        packed = kall[4 * k : 4 * k + 4, 128:].astype(F32)
        swapped = half_swap(packed)
        rows = jnp.concatenate([packed[:, None, :, :64], swapped[:, None, :, :64]], axis=1)
        return rows.reshape(128, 64)

    def latents(k):
        return jnp.concatenate(
            [kall[4 * k : 4 * k + 4, 32 * b : 32 * b + 32].reshape(128, 128) for b in range(4)], axis=1
        )

    def turned_over(k):
        block, turned = latents(k).T, keys(k).T.astype(BF16)
        ktst[k, :, :64] = block.reshape(8, 64, 128)
        ktst[k, :, 64:] = turned.reshape(8, 8, 128)
        return block, turned

    def spread(k):
        to_all_tp(lambda step: (to_tp(ktst.at[k, tp_of(step)], krecv.at[k, tp], k2send, k2rsem.at[k], step),))
        krecv[k, tp] = ktst[k, tp]

    here = []
    for k in range(3):
        arrived(k)
        here.append(turned_over(k))
        spread(k)

    to_tp(aall.at[seven], aall.at[seven], asend, small.at[1], 1).wait_recv()
    absorbed = jnp.concatenate([aall[2 * u] + aall[2 * u + 1] for u in range(4)], axis=1)

    def scores(block, turned):
        total = jnp.dot(absorbed, block, preferred_element_type=F32)
        total += jnp.dot(q_turn, turned, preferred_element_type=F32)
        return total * (192.0 ** -0.5)

    def mixed(weight, k):
        return jnp.dot(weight.astype(BF16), latents(k), preferred_element_type=F32)

    arrived(3)
    final = turned_over(3)
    seen = [scores(*group) for group in here]
    top_seen = jnp.max(jnp.maximum(jnp.maximum(seen[0], seen[1]), seen[2]), axis=1, keepdims=True)
    weights = [jnp.exp(s - top_seen) for s in seen]
    total_seen = jnp.sum(weights[0] + weights[1] + weights[2], axis=1, keepdims=True)
    context_seen = mixed(weights[0], 0) + mixed(weights[1], 1) + mixed(weights[2], 2)

    late = scores(*final)
    top = jnp.maximum(top_seen, jnp.max(late, axis=1, keepdims=True))
    weight = jnp.exp(late - top)
    shrink = jnp.exp(top_seen - top)
    total = total_seen * shrink + jnp.sum(weight, axis=1, keepdims=True)
    context = context_seen * shrink + mixed(weight, 3)
    stats = jnp.where(iota((16, 128), 1) < 64, top, total)
    for t in range(8):
        asc[t, :, :512] = context[2 * t : 2 * t + 2]
        asc[t, :, 512:] = stats[2 * t : 2 * t + 2]
    to_all_tp(lambda step: (to_tp(asc.at[tp_of(step)], arecv.at[tp], csend, small.at[2], step),))
    arecv[tp] = asc[tp]
    spread(3)

    def arrange(k):
        to_tp(ktst.at[k, seven], krecv.at[k, seven], k2send, k2rsem.at[k], 1).wait_recv()
        for a, block, turned in arranged(krecv.at[k]):
            lanes = lanes_of(sp, 4 * k + a)
            stage[:, lanes] = block
            turned_stage[:, lanes] = turned

    for k in range(3):
        arrange(k)

    to_tp(pst.at[seven], pst.at[seven], psend, small.at[0], 1).wait_recv()
    to_tp(asc.at[seven], arecv.at[seven], csend, small.at[2], 1).wait_recv()
    got = arecv[...]
    tops, totals = got[:, :, 512:513], got[:, :, 576:577]
    share = jnp.exp(tops - jnp.max(tops, axis=0, keepdims=True))
    summed = jnp.sum(got[:, :, :512] * share, axis=0) / jnp.sum(totals * share, axis=0)
    summed = jnp.concatenate([summed, jnp.zeros((14, 512), F32)], axis=0).astype(BF16)
    values = jnp.dot(summed, pall[...], preferred_element_type=F32)
    values = jnp.where(iota((16, 128), 0) == 0, values[:, :128], values[:, 128:])[:2]
    values = values * lax.rsqrt(jnp.mean(values * values, axis=1, keepdims=True) + EPS)
    read_out[...] = values.astype(BF16)

    sent = pl.ds(OTHERS, 15)
    to_sp(kst.at[sent], kall.at[sent], ksend, krsem.at[0], OTHERS).wait_send()
    to_tp(qn.at[seven], qn.at[seven], qsend[0], qrsem.at[0], 1).wait_send()
    to_tp(qr.at[seven], qr.at[seven], qsend[1], qrsem.at[1], 1).wait_send()
    to_tp(pst.at[seven], pst.at[seven], psend, small.at[0], 1).wait_send()
    to_tp(aall.at[seven], aall.at[seven], asend, small.at[1], 1).wait_send()
    to_tp(asc.at[seven], arecv.at[seven], csend, small.at[2], 1).wait_send()
    to_tp(ktst.at[:, seven], ktst.at[:, seven], k2send, k2rsem.at[3], 1).wait_send()
    arrange(3)


def finish(stage, turned_stage, read_in, out_s, out_r, out_f, sem):
    pieces = 4
    for n in range(pieces):
        lanes = pl.ds(4096 // pieces * n, 4096 // pieces)
        pltpu.make_async_copy(stage.at[:, lanes], out_s.at[:, lanes], sem.at[0]).start()
    others = [
        pltpu.make_async_copy(turned_stage, out_r, sem.at[1]), pltpu.make_async_copy(read_in, out_f, sem.at[2])
    ]
    for c in others:
        c.start()
    pltpu.make_async_copy(stage, out_s, sem.at[0]).wait()
    for c in others:
        c.wait()


def solution(mesh):
    angles = trig_tables(128, 32, 64)

    def step(x, gain, w, rd, scal, look, payload, qn, qr):
        hbm = pl.BlockSpec(memory_space=pltpu.HBM)
        vmem = pl.BlockSpec(memory_space=pltpu.VMEM)
        dma = pltpu.SemaphoreType.DMA
        received = pl.pallas_call(
            kernel,
            out_shape=(
                jax.ShapeDtypeStruct((64, 4096), BF16),
                jax.ShapeDtypeStruct((8, 4096), BF16),
                jax.ShapeDtypeStruct((2, 128), BF16),
            ),
            in_specs=[hbm] * 10,
            out_specs=(vmem,) * 3,
            scratch_shapes=[
                pltpu.VMEM((16, 32, 2048), BF16),
                pltpu.VMEM((1, 2048), F32),
                pltpu.VMEM((2048, 640), BF16),
                pltpu.VMEM((64, 2048), BF16),
                pltpu.VMEM((1, 512), F32),
                pltpu.VMEM((1024, 128), BF16),
                pltpu.VMEM((1024, 128), BF16),
                pltpu.VMEM((168, 128), F32),
                pltpu.VMEM((16, 144, 128), BF16),
                pltpu.VMEM((16, 144, 128), BF16),
                pltpu.VMEM((8, 2, 128), BF16),
                pltpu.VMEM((8, 2, 64), BF16),
                pltpu.VMEM((8, 16, 128), BF16),
                pltpu.VMEM((8, 64, 256), BF16),
                pltpu.VMEM((512, 256), BF16),
                pltpu.VMEM((4, 8, 72, 128), BF16),
                pltpu.VMEM((4, 8, 72, 128), BF16),
                pltpu.VMEM((8, 2, 640), F32),
                pltpu.VMEM((8, 2, 640), F32),
                pltpu.VMEM((128, 512), F32),
                pltpu.VMEM((128, 2048), BF16),
                dma((2,)),
                dma((9,)),
                dma((4,)),
                dma((2,)),
                dma((3,)),
                dma((4,)),
            ],
            compiler_params=pltpu.CompilerParams(
                collective_id=0, has_side_effects=True, vmem_limit_bytes=48 * 1024 * 1024
            ),
        )(
            *(
                pltpu.with_memory_space_constraint(v, pltpu.HBM)
                for v in (
                    x, gain.reshape(1, 2048), w, rd.T, scal.reshape(1, 512), look.reshape(1024, 128),
                    payload.reshape(1024, 128), qn.reshape(2, 128), qr.reshape(2, 64),
                    jnp.asarray(angles),
                )
            )
        )
        stored, rotary, read = pl.pallas_call(
            finish,
            out_shape=(
                jax.ShapeDtypeStruct((64, 4096), BF16),
                jax.ShapeDtypeStruct((8, 4096), BF16),
                jax.ShapeDtypeStruct((2, 128), BF16),
            ),
            in_specs=[vmem] * 3,
            out_specs=(hbm,) * 3,
            scratch_shapes=[dma((3,))],
        )(*(pltpu.with_memory_space_constraint(v, pltpu.VMEM) for v in received))
        return stored.T[None], rotary.T[None], read[None]

    tp = "tp"
    both = ("sp", "tp")
    in_specs = (
        P(None, both, None), P(), P(), P(), P(), P(tp, None, None), P(tp, None, None),
        P("sp", tp, None), P("sp", tp, None),
    )
    out_specs = (P("sp", None, tp), P("sp", None, tp), P("sp", tp, None))
    return jax.shard_map(step, mesh=mesh, in_specs=in_specs, out_specs=out_specs, check_vma=False)
```

```python
import jax
import jax.numpy as jnp
import numpy as np
from jax import lax
from jax.experimental import pallas as pl
from jax.experimental.pallas import tpu as pltpu
from jax.sharding import PartitionSpec as P

MESH = pl.DeviceIdType.MESH
EPS = 1e-6
ROPE_BASE = 10000.0
F32 = jnp.float32
BF16 = jnp.bfloat16

NT = (((1,), (1,)), ((), ()))

STEPS = (
    (2, 0), (0, 2), (1, 1), (3, 3),
    (1, 2), (3, 2), (1, 3), (3, 1),
    (2, 1), (2, 3), (1, 0), (3, 0),
    (2, 2), (0, 1), (0, 3), (0, 0),
)
OWN = STEPS.index((0, 0))
OTHERS = 1 if OWN == 0 else 0


def trig_tables(blocks, rows, rope):
    half = rope // 2
    freq = 1.0 / ROPE_BASE ** (np.arange(half, dtype=np.float64) * 2.0 / rope)
    freq = np.concatenate([freq, freq])
    first = np.arange(blocks + 8, dtype=np.float64)[:, None] * rows * freq
    offset = np.arange(rows, dtype=np.float64)[:, None] * freq

    def both(angle):
        return np.concatenate([np.cos(angle), np.sin(angle)], axis=1).astype(np.float32)

    return np.concatenate([both(first), both(offset)], axis=0)


def half_swap(v):
    half = v.shape[-1] // 2
    return jnp.concatenate([v[..., half:], v[..., :half]], axis=-1)


def iota(shape, dim):
    return lax.broadcasted_iota(jnp.int32, shape, dim)


def sp_at(sp, dz, dy):
    return lax.rem(sp // 4 + dz, 4) * 4 + lax.rem(lax.rem(sp, 4) + dy, 4)


def lanes_of(sp, n):
    dz, dy = STEPS[n]
    return pl.ds(pl.multiple_of(256 * sp_at(sp, (4 - dz) % 4, (4 - dy) % 4), 256), 256)


def arranged(source):
    blocks = [source[t].astype(F32) for t in range(8)]
    lane = jnp.right_shift(iota((72, 128), 1), 5)
    for a in range(4):
        mine = [jnp.bitwise_and(lane - a, 3) == j for j in range(3)]
        halves = []
        for u in range(2):
            b = blocks[4 * u : 4 * u + 4]
            v = jnp.where(mine[0], b[0], jnp.where(mine[1], b[1], jnp.where(mine[2], b[2], b[3])))
            halves.append(pltpu.roll(v, 128 - 32 * a, 1) if a else v)
        both = jnp.concatenate(halves, axis=1)
        yield a, both[:64].astype(BF16), both[64:].astype(BF16)


def kernel(
    x_hbm, gain_hbm, w_hbm, rd_hbm, scal_hbm, look_hbm, pay_hbm, qn_hbm, qr_hbm, tab_hbm,
    stage, turned_stage, read_out,
    xb, gain, w, rd, scal, look, pay, tab,
    kst, kall, qn, qr, aall, pst, pall, ktst, krecv, asc, arecv, part, held,
    xsem, wsem, krsem, qrsem, small, k2rsem,
):
    sp, tp = lax.axis_index("sp"), lax.axis_index("tp")

    def tp_of(step):
        return lax.rem(tp + step, 8)

    ksend, k2send, psend, asend, csend = (wsem.at[n] for n in (1, 2, 4, 5, 6))
    qsend = (wsem.at[3], wsem.at[7])

    barrier = pltpu.get_barrier_semaphore()
    steps = sorted(STEPS, key=lambda s: -min(s[0], 4 - s[0]) - min(s[1], 4 - s[1]))[:15]

    def greet(some):
        for dz, dy in some:
            pl.semaphore_signal(barrier, inc=1, device_id=(sp_at(sp, dz, dy), tp), device_id_type=MESH)


    halves = [pl.ds(0, 1024), pl.ds(1024, 1024)]
    loads = [
        pltpu.make_async_copy(src, dst, wsem.at[n % 9])
        for n, (src, dst) in enumerate(
            (
                (gain_hbm, gain), (w_hbm.at[halves[0]], w.at[halves[0], pl.ds(0, 512)]),
                (w_hbm.at[halves[1]], w.at[halves[1], pl.ds(0, 512)]),
                (rd_hbm, rd), (scal_hbm, scal), (tab_hbm, tab),
                (pay_hbm, pay), (qn_hbm, qn.at[tp]), (qr_hbm, qr.at[tp]), (look_hbm, look),
            )
        )
    ]
    for n in (6, 5, 0, 7, 8, 3):
        loads[n].start()
    for n in range(4):
        pltpu.make_async_copy(x_hbm.at[sp_at(sp, *STEPS[n])], xb.at[n], xsem.at[0]).start()
    loads[1].start()

    greet(steps)
    for step in (4, 5, 3, 2, 6, 7, 1):
        pl.semaphore_signal(barrier, inc=1, device_id=(sp, tp_of(step)), device_id_type=MESH)
    for n in (4, 2):
        loads[n].start()

    def to_tp(src, dst, send, recv, step):
        return pltpu.make_async_remote_copy(
            src_ref=src, dst_ref=dst, send_sem=send, recv_sem=recv,
            device_id=(sp, tp_of(step)), device_id_type=MESH,
        )

    def to_all_tp(copies):
        for step in (4, 5, 3, 2, 6, 7, 1):
            for c in copies(step):
                c.start()

    def to_sp(src, dst, send, recv, n):
        return pltpu.make_async_remote_copy(
            src_ref=src, dst_ref=dst, send_sem=send, recv_sem=recv,
            device_id=(sp_at(sp, *STEPS[n]), tp), device_id_type=MESH,
        )

    row, col = iota((256, 256), 0), iota((256, 256), 1)
    wanted = jnp.bitwise_and(row, 15) * 16 + jnp.right_shift(row, 4)
    order = jnp.where(col == wanted, 1.0, 0.0).astype(BF16)
    loads[6].wait()
    for g in range(4):
        rows = jnp.dot(order, pay[256 * g : 256 * (g + 1), :], preferred_element_type=F32)
        rows = rows.astype(BF16).reshape(8, 2, 16, 128)
        for head in range(2):
            pst[:, 16 * g : 16 * (g + 1), 128 * head : 128 * (head + 1)] = rows[:, head]
    mine = pl.ds(pl.multiple_of(tp * 64, 64), 64)
    pall[mine, :] = pst[tp]

    loads[5].wait()
    sign = jnp.where(iota((32, 64), 1) < 32, -1.0, 1.0).astype(F32)
    base = tab[pl.ds(sp * 8 + tp, 1), :]
    offs = tab[136:]
    cos = base[:, :64] * offs[:, :64] - base[:, 64:] * offs[:, 64:]
    sin = (base[:, 64:] * offs[:, :64] + base[:, :64] * offs[:, 64:]) * sign
    loads[0].wait()

    loads[3].wait()
    w[:, 512:] = jnp.concatenate([rd[...].T, jnp.zeros((2048, 64), BF16)], axis=1)

    def project(k, groups):
        count = 4 * groups
        for n in range(groups):
            at = pl.ds(4 * (k + n), 4)
            pltpu.make_async_copy(x_hbm.at[pl.ds(0, 4)], xb.at[at], xsem.at[(k + n) % 2]).wait()
        if k == 1:
            for n in range(12, 16):
                pltpu.make_async_copy(x_hbm.at[sp_at(sp, *STEPS[n])], xb.at[n], xsem.at[n // 4 % 2]).start()
        xv = xb[4 * k : 4 * k + count].reshape(32 * count, 2048).astype(F32)
        scale = lax.rsqrt(jnp.mean(xv * xv, axis=1, keepdims=True) + EPS)
        normed = (xv * scale * gain[...]).astype(BF16)
        if k == 0:
            rot = jnp.dot(normed, w[:, 512:], preferred_element_type=F32)
        else:
            both = jnp.dot(normed, w[...], preferred_element_type=F32)
            latent, rot = both[:, :512], both[:, 512:]
        rot = rot[:, :64].astype(BF16).astype(F32)
        turn = [jnp.concatenate([part] * count, axis=0) for part in (cos, sin)]
        turned = (rot * turn[0] + half_swap(rot) * turn[1]).reshape(count, 2, 16, 64)
        turned = jnp.concatenate([turned[:, 0], turned[:, 1]], axis=-1).astype(BF16)
        kst[4 * k : 4 * k + count, 128:] = turned
        if k == 0:
            loads[1].wait()
            for n in range(4, 8):
                pltpu.make_async_copy(x_hbm.at[sp_at(sp, *STEPS[n])], xb.at[n], xsem.at[n // 4 % 2]).start()
            part[...] = jnp.dot(normed[:, :1024], w[:1024, :512], preferred_element_type=F32)
            held[...] = normed

            @pl.when(sp >= 0)
            def _():
                for n in (2, 4):
                    loads[n].wait()
                loads[9].start()
                for n in range(8, 12):
                    pltpu.make_async_copy(x_hbm.at[sp_at(sp, *STEPS[n])], xb.at[n], xsem.at[n // 4 % 2]).start()

            normed = held[...]
            latent = part[...] + jnp.dot(normed[:, 1024:], w[1024:, :512], preferred_element_type=F32)
        latent = latent.astype(BF16).astype(F32)
        scale = lax.rsqrt(jnp.mean(latent * latent, axis=1, keepdims=True) + EPS)
        stored = (latent * scale * scal[...]).astype(BF16).reshape(count, 32, 512)
        for b in range(4):
            kst[4 * k : 4 * k + count, 32 * b : 32 * b + 32] = stored[:, :, 128 * b : 128 * b + 128]
        if 4 * k <= OWN < 4 * k + count:
            slot = OWN // 4 * 4 + lax.rem(OWN + tp, 4)
            kall[slot] = kst[OWN]
        if k == 0:
            pl.semaphore_wait(barrier, 22)
        for n in range(4 * k, 4 * k + count):
            if n != OWN:
                slot = n // 4 * 4 + lax.rem(n + tp, 4)
                to_sp(kst.at[n], kall.at[slot], ksend, krsem.at[n // 4], n).start()

    def arrived(k):
        count = 4 if k != OWN // 4 else 3
        at = pl.ds(4 * k, count)
        to_sp(kst.at[at], kall.at[at], ksend, krsem.at[k], OTHERS).wait_recv()

    for n in (7, 8):
        loads[n].wait()
    project(0, 1)
    to_all_tp(
        lambda step: (
            to_tp(qn.at[tp], qn.at[tp], qsend[0], qrsem.at[0], step),
            to_tp(qr.at[tp], qr.at[tp], qsend[1], qrsem.at[1], step),
        )
    )
    to_all_tp(lambda step: (to_tp(pst.at[tp_of(step)], pall.at[mine, :], psend, small.at[0], step),))
    project(1, 1)

    project(2, 1)
    project(3, 1)

    loads[9].wait()
    seven = pl.ds(0, 7)
    to_tp(qn.at[seven], qn.at[seven], qsend[0], qrsem.at[0], 1).wait_recv()
    to_tp(qr.at[seven], qr.at[seven], qsend[1], qrsem.at[1], 1).wait_recv()
    q_all = qn[...].astype(F32).reshape(16, 128).astype(BF16)
    t_all = qr[...].astype(F32).reshape(16, 64)
    parts = lax.dot_general(q_all, look[...], NT, preferred_element_type=F32)
    same = jnp.bitwise_and(iota((16, 1024), 1), 15) == iota((16, 1024), 0)
    parts = jnp.where(same, parts, 0.0).astype(BF16)
    pick = jnp.right_shift(iota((1024, 128), 0), 4) + 64 * lax.rem(tp, 2) == iota((1024, 128), 1)
    pick = jnp.where(pick, 1.0, 0.0).astype(BF16)
    aall[tp] = jnp.dot(parts, pick, preferred_element_type=F32).astype(BF16)
    to_all_tp(lambda step: (to_tp(aall.at[tp], aall.at[tp], asend, small.at[1], step),))
    last = tab[128:129, :]
    q_turn = (t_all * last[:, :64] + half_swap(t_all) * (last[:, 64:] * sign[:1])).astype(BF16)

    def keys(k):
        packed = kall[4 * k : 4 * k + 4, 128:].astype(F32)
        swapped = half_swap(packed)
        rows = jnp.concatenate([packed[:, None, :, :64], swapped[:, None, :, :64]], axis=1)
        return rows.reshape(128, 64)

    def latents(k):
        return jnp.concatenate(
            [kall[4 * k : 4 * k + 4, 32 * b : 32 * b + 32].reshape(128, 128) for b in range(4)], axis=1
        )

    def turned_over(k):
        block, turned = latents(k).T, keys(k).T.astype(BF16)
        ktst[k, :, :64] = block.reshape(8, 64, 128)
        ktst[k, :, 64:] = turned.reshape(8, 8, 128)
        return block, turned

    def spread(k):
        to_all_tp(lambda step: (to_tp(ktst.at[k, tp_of(step)], krecv.at[k, tp], k2send, k2rsem.at[k], step),))
        krecv[k, tp] = ktst[k, tp]

    here = []
    for k in range(3):
        arrived(k)
        here.append(turned_over(k))
        spread(k)

    to_tp(aall.at[seven], aall.at[seven], asend, small.at[1], 1).wait_recv()
    absorbed = jnp.concatenate([aall[2 * u] + aall[2 * u + 1] for u in range(4)], axis=1)

    def scores(block, turned):
        total = jnp.dot(absorbed, block, preferred_element_type=F32)
        total += jnp.dot(q_turn, turned, preferred_element_type=F32)
        return total * (192.0 ** -0.5)

    def mixed(weight, k):
        return jnp.dot(weight.astype(BF16), latents(k), preferred_element_type=F32)

    seen = [scores(*group) for group in here]
    top_seen = jnp.max(jnp.maximum(jnp.maximum(seen[0], seen[1]), seen[2]), axis=1, keepdims=True)
    weights = [jnp.exp(s - top_seen) for s in seen]
    total_seen = jnp.sum(weights[0] + weights[1] + weights[2], axis=1, keepdims=True)
    context_seen = mixed(weights[0], 0) + mixed(weights[1], 1) + mixed(weights[2], 2)

    arrived(3)
    late = scores(*turned_over(3))
    top = jnp.maximum(top_seen, jnp.max(late, axis=1, keepdims=True))
    weight = jnp.exp(late - top)
    shrink = jnp.exp(top_seen - top)
    total = total_seen * shrink + jnp.sum(weight, axis=1, keepdims=True)
    context = context_seen * shrink + mixed(weight, 3)
    stats = jnp.where(iota((16, 128), 1) < 64, top, total)
    for t in range(8):
        asc[t, :, :512] = context[2 * t : 2 * t + 2]
        asc[t, :, 512:] = stats[2 * t : 2 * t + 2]
    to_all_tp(lambda step: (to_tp(asc.at[tp_of(step)], arecv.at[tp], csend, small.at[2], step),))
    arecv[tp] = asc[tp]
    spread(3)

    def arrange(k):
        to_tp(ktst.at[k, seven], krecv.at[k, seven], k2send, k2rsem.at[k], 1).wait_recv()
        for a, block, turned in arranged(krecv.at[k]):
            lanes = lanes_of(sp, 4 * k + a)
            stage[:, lanes] = block
            turned_stage[:, lanes] = turned

    for k in range(3):
        arrange(k)

    to_tp(pst.at[seven], pst.at[seven], psend, small.at[0], 1).wait_recv()
    to_tp(asc.at[seven], arecv.at[seven], csend, small.at[2], 1).wait_recv()
    got = arecv[...]
    tops, totals = got[:, :, 512:513], got[:, :, 576:577]
    share = jnp.exp(tops - jnp.max(tops, axis=0, keepdims=True))
    summed = jnp.sum(got[:, :, :512] * share, axis=0) / jnp.sum(totals * share, axis=0)
    summed = jnp.concatenate([summed, jnp.zeros((14, 512), F32)], axis=0).astype(BF16)
    values = jnp.dot(summed, pall[...], preferred_element_type=F32)
    values = jnp.where(iota((16, 128), 0) == 0, values[:, :128], values[:, 128:])[:2]
    values = values * lax.rsqrt(jnp.mean(values * values, axis=1, keepdims=True) + EPS)
    read_out[...] = values.astype(BF16)

    sent = pl.ds(OTHERS, 15)
    to_sp(kst.at[sent], kall.at[sent], ksend, krsem.at[0], OTHERS).wait_send()
    to_tp(qn.at[seven], qn.at[seven], qsend[0], qrsem.at[0], 1).wait_send()
    to_tp(qr.at[seven], qr.at[seven], qsend[1], qrsem.at[1], 1).wait_send()
    to_tp(pst.at[seven], pst.at[seven], psend, small.at[0], 1).wait_send()
    to_tp(aall.at[seven], aall.at[seven], asend, small.at[1], 1).wait_send()
    to_tp(asc.at[seven], arecv.at[seven], csend, small.at[2], 1).wait_send()
    to_tp(ktst.at[:, seven], ktst.at[:, seven], k2send, k2rsem.at[3], 1).wait_send()
    arrange(3)


def finish(stage, turned_stage, read_in, out_s, out_r, out_f, sem):
    pieces = 4
    for n in range(pieces):
        lanes = pl.ds(4096 // pieces * n, 4096 // pieces)
        pltpu.make_async_copy(stage.at[:, lanes], out_s.at[:, lanes], sem.at[0]).start()
    others = [
        pltpu.make_async_copy(turned_stage, out_r, sem.at[1]), pltpu.make_async_copy(read_in, out_f, sem.at[2])
    ]
    for c in others:
        c.start()
    pltpu.make_async_copy(stage, out_s, sem.at[0]).wait()
    for c in others:
        c.wait()


def solution(mesh):
    angles = trig_tables(128, 32, 64)

    def step(x, gain, w, rd, scal, look, payload, qn, qr):
        hbm = pl.BlockSpec(memory_space=pltpu.HBM)
        vmem = pl.BlockSpec(memory_space=pltpu.VMEM)
        dma = pltpu.SemaphoreType.DMA
        received = pl.pallas_call(
            kernel,
            out_shape=(
                jax.ShapeDtypeStruct((64, 4096), BF16),
                jax.ShapeDtypeStruct((8, 4096), BF16),
                jax.ShapeDtypeStruct((2, 128), BF16),
            ),
            in_specs=[hbm] * 10,
            out_specs=(vmem,) * 3,
            scratch_shapes=[
                pltpu.VMEM((16, 32, 2048), BF16),
                pltpu.VMEM((1, 2048), F32),
                pltpu.VMEM((2048, 640), BF16),
                pltpu.VMEM((64, 2048), BF16),
                pltpu.VMEM((1, 512), F32),
                pltpu.VMEM((1024, 128), BF16),
                pltpu.VMEM((1024, 128), BF16),
                pltpu.VMEM((168, 128), F32),
                pltpu.VMEM((16, 144, 128), BF16),
                pltpu.VMEM((16, 144, 128), BF16),
                pltpu.VMEM((8, 2, 128), BF16),
                pltpu.VMEM((8, 2, 64), BF16),
                pltpu.VMEM((8, 16, 128), BF16),
                pltpu.VMEM((8, 64, 256), BF16),
                pltpu.VMEM((512, 256), BF16),
                pltpu.VMEM((4, 8, 72, 128), BF16),
                pltpu.VMEM((4, 8, 72, 128), BF16),
                pltpu.VMEM((8, 2, 640), F32),
                pltpu.VMEM((8, 2, 640), F32),
                pltpu.VMEM((128, 512), F32),
                pltpu.VMEM((128, 2048), BF16),
                dma((2,)),
                dma((9,)),
                dma((4,)),
                dma((2,)),
                dma((3,)),
                dma((4,)),
            ],
            compiler_params=pltpu.CompilerParams(
                collective_id=0, has_side_effects=True, vmem_limit_bytes=48 * 1024 * 1024
            ),
        )(
            *(
                pltpu.with_memory_space_constraint(v, pltpu.HBM)
                for v in (
                    x, gain.reshape(1, 2048), w, rd.T, scal.reshape(1, 512), look.reshape(1024, 128),
                    payload.reshape(1024, 128), qn.reshape(2, 128), qr.reshape(2, 64),
                    jnp.asarray(angles),
                )
            )
        )
        stored, rotary, read = pl.pallas_call(
            finish,
            out_shape=(
                jax.ShapeDtypeStruct((64, 4096), BF16),
                jax.ShapeDtypeStruct((8, 4096), BF16),
                jax.ShapeDtypeStruct((2, 128), BF16),
            ),
            in_specs=[vmem] * 3,
            out_specs=(hbm,) * 3,
            scratch_shapes=[dma((3,))],
        )(*(pltpu.with_memory_space_constraint(v, pltpu.VMEM) for v in received))
        return stored.T[None], rotary.T[None], read[None]

    tp = "tp"
    both = ("sp", "tp")
    in_specs = (
        P(None, both, None), P(), P(), P(), P(), P(tp, None, None), P(tp, None, None),
        P("sp", tp, None), P("sp", tp, None),
    )
    out_specs = (P("sp", None, tp), P("sp", None, tp), P("sp", tp, None))
    return jax.shard_map(step, mesh=mesh, in_specs=in_specs, out_specs=out_specs, check_vma=False)
```

```python
import jax
import jax.numpy as jnp
import numpy as np
from jax import lax
from jax.experimental import pallas as pl
from jax.experimental.pallas import tpu as pltpu
from jax.sharding import PartitionSpec as P

MESH = pl.DeviceIdType.MESH
EPS = 1e-6
ROPE_BASE = 10000.0
F32 = jnp.float32
BF16 = jnp.bfloat16

NT = (((1,), (1,)), ((), ()))

STEPS = (
    (2, 0), (0, 2), (1, 1), (3, 3),
    (1, 2), (3, 2), (1, 3), (3, 1),
    (2, 1), (2, 3), (1, 0), (3, 0),
    (2, 2), (0, 1), (0, 3), (0, 0),
)
OWN = STEPS.index((0, 0))
OTHERS = 1 if OWN == 0 else 0


def trig_tables(blocks, rows, rope):
    half = rope // 2
    freq = 1.0 / ROPE_BASE ** (np.arange(half, dtype=np.float64) * 2.0 / rope)
    freq = np.concatenate([freq, freq])
    first = np.arange(blocks + 8, dtype=np.float64)[:, None] * rows * freq
    offset = np.arange(rows, dtype=np.float64)[:, None] * freq

    def both(angle):
        return np.concatenate([np.cos(angle), np.sin(angle)], axis=1).astype(np.float32)

    return np.concatenate([both(first), both(offset)], axis=0)


def half_swap(v):
    half = v.shape[-1] // 2
    return jnp.concatenate([v[..., half:], v[..., :half]], axis=-1)


def iota(shape, dim):
    return lax.broadcasted_iota(jnp.int32, shape, dim)


def sp_at(sp, dz, dy):
    return lax.rem(sp // 4 + dz, 4) * 4 + lax.rem(lax.rem(sp, 4) + dy, 4)


def lanes_of(sp, n):
    dz, dy = STEPS[n]
    return pl.ds(pl.multiple_of(256 * sp_at(sp, (4 - dz) % 4, (4 - dy) % 4), 256), 256)


def arranged(source):
    blocks = [source[t].astype(F32) for t in range(8)]
    lane = jnp.right_shift(iota((72, 128), 1), 5)
    for a in range(4):
        mine = [jnp.bitwise_and(lane - a, 3) == j for j in range(3)]
        halves = []
        for u in range(2):
            b = blocks[4 * u : 4 * u + 4]
            v = jnp.where(mine[0], b[0], jnp.where(mine[1], b[1], jnp.where(mine[2], b[2], b[3])))
            halves.append(pltpu.roll(v, 128 - 32 * a, 1) if a else v)
        both = jnp.concatenate(halves, axis=1)
        yield a, both[:64].astype(BF16), both[64:].astype(BF16)


def kernel(
    x_hbm, gain_hbm, w_hbm, rd_hbm, scal_hbm, look_hbm, pay_hbm, qn_hbm, qr_hbm, tab_hbm,
    stage, turned_stage, read_out,
    xb, gain, w, rd, scal, look, pay, tab,
    kst, kall, qn, qr, aall, pst, pall, ktst, krecv, asc, arecv, part, held,
    xsem, wsem, krsem, qrsem, small, k2rsem,
):
    sp, tp = lax.axis_index("sp"), lax.axis_index("tp")

    def tp_of(step):
        return lax.rem(tp + step, 8)

    ksend, k2send, psend, asend, csend = (wsem.at[n] for n in (1, 2, 4, 5, 6))
    qsend = (wsem.at[3], wsem.at[7])

    barrier = pltpu.get_barrier_semaphore()
    steps = sorted(STEPS, key=lambda s: -min(s[0], 4 - s[0]) - min(s[1], 4 - s[1]))[:15]

    def greet(some):
        for dz, dy in some:
            pl.semaphore_signal(barrier, inc=1, device_id=(sp_at(sp, dz, dy), tp), device_id_type=MESH)

    greet(steps[:5])

    halves = [pl.ds(0, 1024), pl.ds(1024, 1024)]
    loads = [
        pltpu.make_async_copy(src, dst, wsem.at[n % 9])
        for n, (src, dst) in enumerate(
            (
                (gain_hbm, gain), (w_hbm.at[halves[0]], w.at[halves[0], pl.ds(0, 512)]),
                (w_hbm.at[halves[1]], w.at[halves[1], pl.ds(0, 512)]),
                (rd_hbm, rd), (scal_hbm, scal), (tab_hbm, tab),
                (pay_hbm, pay), (qn_hbm, qn.at[tp]), (qr_hbm, qr.at[tp]), (look_hbm, look),
            )
        )
    ]
    for n in (6, 5, 0, 7, 8, 3):
        loads[n].start()
    for n in range(4):
        pltpu.make_async_copy(x_hbm.at[sp_at(sp, *STEPS[n])], xb.at[n], xsem.at[0]).start()
    loads[1].start()

    greet(steps[5:])
    for step in (4, 5, 3, 2, 6, 7, 1):
        pl.semaphore_signal(barrier, inc=1, device_id=(sp, tp_of(step)), device_id_type=MESH)
    for n in (4, 2):
        loads[n].start()

    def to_tp(src, dst, send, recv, step):
        return pltpu.make_async_remote_copy(
            src_ref=src, dst_ref=dst, send_sem=send, recv_sem=recv,
            device_id=(sp, tp_of(step)), device_id_type=MESH,
        )

    def to_all_tp(copies):
        for step in (3, 5, 4, 6, 2, 7, 1):
            for c in copies(step):
                c.start()

    def to_sp(src, dst, send, recv, n):
        return pltpu.make_async_remote_copy(
            src_ref=src, dst_ref=dst, send_sem=send, recv_sem=recv,
            device_id=(sp_at(sp, *STEPS[n]), tp), device_id_type=MESH,
        )

    row, col = iota((256, 256), 0), iota((256, 256), 1)
    wanted = jnp.bitwise_and(row, 15) * 16 + jnp.right_shift(row, 4)
    order = jnp.where(col == wanted, 1.0, 0.0).astype(BF16)
    loads[6].wait()
    for g in range(4):
        rows = jnp.dot(order, pay[256 * g : 256 * (g + 1), :], preferred_element_type=F32)
        rows = rows.astype(BF16).reshape(8, 2, 16, 128)
        for head in range(2):
            pst[:, 16 * g : 16 * (g + 1), 128 * head : 128 * (head + 1)] = rows[:, head]
    mine = pl.ds(pl.multiple_of(tp * 64, 64), 64)
    pall[mine, :] = pst[tp]

    loads[5].wait()
    sign = jnp.where(iota((32, 64), 1) < 32, -1.0, 1.0).astype(F32)
    base = tab[pl.ds(sp * 8 + tp, 1), :]
    offs = tab[136:]
    cos = base[:, :64] * offs[:, :64] - base[:, 64:] * offs[:, 64:]
    sin = (base[:, 64:] * offs[:, :64] + base[:, :64] * offs[:, 64:]) * sign
    loads[0].wait()

    loads[3].wait()
    w[:, 512:] = jnp.concatenate([rd[...].T, jnp.zeros((2048, 64), BF16)], axis=1)

    def project(k, groups):
        count = 4 * groups
        for n in range(groups):
            at = pl.ds(4 * (k + n), 4)
            pltpu.make_async_copy(x_hbm.at[pl.ds(0, 4)], xb.at[at], xsem.at[(k + n) % 2]).wait()
        if k == 1:
            for n in range(12, 16):
                pltpu.make_async_copy(x_hbm.at[sp_at(sp, *STEPS[n])], xb.at[n], xsem.at[n // 4 % 2]).start()
        xv = xb[4 * k : 4 * k + count].reshape(32 * count, 2048).astype(F32)
        scale = lax.rsqrt(jnp.mean(xv * xv, axis=1, keepdims=True) + EPS)
        normed = (xv * scale * gain[...]).astype(BF16)
        if k == 0:
            rot = jnp.dot(normed, w[:, 512:], preferred_element_type=F32)
        else:
            both = jnp.dot(normed, w[...], preferred_element_type=F32)
            latent, rot = both[:, :512], both[:, 512:]
        rot = rot[:, :64].astype(BF16).astype(F32)
        turn = [jnp.concatenate([part] * count, axis=0) for part in (cos, sin)]
        turned = (rot * turn[0] + half_swap(rot) * turn[1]).reshape(count, 2, 16, 64)
        turned = jnp.concatenate([turned[:, 0], turned[:, 1]], axis=-1).astype(BF16)
        kst[4 * k : 4 * k + count, 128:] = turned
        if k == 0:
            loads[1].wait()
            for n in range(4, 8):
                pltpu.make_async_copy(x_hbm.at[sp_at(sp, *STEPS[n])], xb.at[n], xsem.at[n // 4 % 2]).start()
            part[...] = jnp.dot(normed[:, :1024], w[:1024, :512], preferred_element_type=F32)
            held[...] = normed

            @pl.when(sp >= 0)
            def _():
                for n in (2, 4):
                    loads[n].wait()
                loads[9].start()
                for n in range(8, 12):
                    pltpu.make_async_copy(x_hbm.at[sp_at(sp, *STEPS[n])], xb.at[n], xsem.at[n // 4 % 2]).start()

            normed = held[...]
            latent = part[...] + jnp.dot(normed[:, 1024:], w[1024:, :512], preferred_element_type=F32)
        latent = latent.astype(BF16).astype(F32)
        scale = lax.rsqrt(jnp.mean(latent * latent, axis=1, keepdims=True) + EPS)
        stored = (latent * scale * scal[...]).astype(BF16).reshape(count, 32, 512)
        for b in range(4):
            kst[4 * k : 4 * k + count, 32 * b : 32 * b + 32] = stored[:, :, 128 * b : 128 * b + 128]
        if 4 * k <= OWN < 4 * k + count:
            slot = OWN // 4 * 4 + lax.rem(OWN + tp, 4)
            kall[slot] = kst[OWN]
        if k == 0:
            pl.semaphore_wait(barrier, 22)
        for n in range(4 * k, 4 * k + count):
            if n != OWN:
                slot = n // 4 * 4 + lax.rem(n + tp, 4)
                to_sp(kst.at[n], kall.at[slot], ksend, krsem.at[n // 4], n).start()

    def arrived(k):
        count = 4 if k != OWN // 4 else 3
        at = pl.ds(4 * k, count)
        to_sp(kst.at[at], kall.at[at], ksend, krsem.at[k], OTHERS).wait_recv()

    for n in (7, 8):
        loads[n].wait()
    project(0, 1)
    to_all_tp(
        lambda step: (
            to_tp(qn.at[tp], qn.at[tp], qsend[0], qrsem.at[0], step),
            to_tp(qr.at[tp], qr.at[tp], qsend[1], qrsem.at[1], step),
        )
    )
    to_all_tp(lambda step: (to_tp(pst.at[tp_of(step)], pall.at[mine, :], psend, small.at[0], step),))
    project(1, 1)

    project(2, 1)
    project(3, 1)

    loads[9].wait()
    seven = pl.ds(0, 7)
    to_tp(qn.at[seven], qn.at[seven], qsend[0], qrsem.at[0], 1).wait_recv()
    to_tp(qr.at[seven], qr.at[seven], qsend[1], qrsem.at[1], 1).wait_recv()
    q_all = qn[...].astype(F32).reshape(16, 128).astype(BF16)
    t_all = qr[...].astype(F32).reshape(16, 64)
    parts = lax.dot_general(q_all, look[...], NT, preferred_element_type=F32)
    same = jnp.bitwise_and(iota((16, 1024), 1), 15) == iota((16, 1024), 0)
    parts = jnp.where(same, parts, 0.0).astype(BF16)
    pick = jnp.right_shift(iota((1024, 128), 0), 4) + 64 * lax.rem(tp, 2) == iota((1024, 128), 1)
    pick = jnp.where(pick, 1.0, 0.0).astype(BF16)
    aall[tp] = jnp.dot(parts, pick, preferred_element_type=F32).astype(BF16)
    to_all_tp(lambda step: (to_tp(aall.at[tp], aall.at[tp], asend, small.at[1], step),))
    last = tab[128:129, :]
    q_turn = (t_all * last[:, :64] + half_swap(t_all) * (last[:, 64:] * sign[:1])).astype(BF16)

    def keys(k):
        packed = kall[4 * k : 4 * k + 4, 128:].astype(F32)
        swapped = half_swap(packed)
        rows = jnp.concatenate([packed[:, None, :, :64], swapped[:, None, :, :64]], axis=1)
        return rows.reshape(128, 64)

    def latents(k):
        return jnp.concatenate(
            [kall[4 * k : 4 * k + 4, 32 * b : 32 * b + 32].reshape(128, 128) for b in range(4)], axis=1
        )

    def turned_over(k):
        block, turned = latents(k).T, keys(k).T.astype(BF16)
        ktst[k, :, :64] = block.reshape(8, 64, 128)
        ktst[k, :, 64:] = turned.reshape(8, 8, 128)
        return block, turned

    def spread(k):
        to_all_tp(lambda step: (to_tp(ktst.at[k, tp_of(step)], krecv.at[k, tp], k2send, k2rsem.at[k], step),))
        krecv[k, tp] = ktst[k, tp]

    here = []
    for k in range(3):
        arrived(k)
        here.append(turned_over(k))
        spread(k)

    to_tp(aall.at[seven], aall.at[seven], asend, small.at[1], 1).wait_recv()
    absorbed = jnp.concatenate([aall[2 * u] + aall[2 * u + 1] for u in range(4)], axis=1)

    def scores(block, turned):
        total = jnp.dot(absorbed, block, preferred_element_type=F32)
        total += jnp.dot(q_turn, turned, preferred_element_type=F32)
        return total * (192.0 ** -0.5)

    def mixed(weight, k):
        return jnp.dot(weight.astype(BF16), latents(k), preferred_element_type=F32)

    seen = [scores(*group) for group in here]
    top_seen = jnp.max(jnp.maximum(jnp.maximum(seen[0], seen[1]), seen[2]), axis=1, keepdims=True)
    weights = [jnp.exp(s - top_seen) for s in seen]
    total_seen = jnp.sum(weights[0] + weights[1] + weights[2], axis=1, keepdims=True)
    context_seen = mixed(weights[0], 0) + mixed(weights[1], 1) + mixed(weights[2], 2)

    arrived(3)
    late = scores(*turned_over(3))
    top = jnp.maximum(top_seen, jnp.max(late, axis=1, keepdims=True))
    weight = jnp.exp(late - top)
    shrink = jnp.exp(top_seen - top)
    total = total_seen * shrink + jnp.sum(weight, axis=1, keepdims=True)
    context = context_seen * shrink + mixed(weight, 3)
    stats = jnp.where(iota((16, 128), 1) < 64, top, total)
    for t in range(8):
        asc[t, :, :512] = context[2 * t : 2 * t + 2]
        asc[t, :, 512:] = stats[2 * t : 2 * t + 2]
    to_all_tp(lambda step: (to_tp(asc.at[tp_of(step)], arecv.at[tp], csend, small.at[2], step),))
    arecv[tp] = asc[tp]
    spread(3)

    def arrange(k):
        to_tp(ktst.at[k, seven], krecv.at[k, seven], k2send, k2rsem.at[k], 1).wait_recv()
        for a, block, turned in arranged(krecv.at[k]):
            lanes = lanes_of(sp, 4 * k + a)
            stage[:, lanes] = block
            turned_stage[:, lanes] = turned

    for k in range(3):
        arrange(k)

    to_tp(pst.at[seven], pst.at[seven], psend, small.at[0], 1).wait_recv()
    to_tp(asc.at[seven], arecv.at[seven], csend, small.at[2], 1).wait_recv()
    got = arecv[...]
    tops, totals = got[:, :, 512:513], got[:, :, 576:577]
    share = jnp.exp(tops - jnp.max(tops, axis=0, keepdims=True))
    summed = jnp.sum(got[:, :, :512] * share, axis=0) / jnp.sum(totals * share, axis=0)
    summed = jnp.concatenate([summed, jnp.zeros((14, 512), F32)], axis=0).astype(BF16)
    values = jnp.dot(summed, pall[...], preferred_element_type=F32)
    values = jnp.where(iota((16, 128), 0) == 0, values[:, :128], values[:, 128:])[:2]
    values = values * lax.rsqrt(jnp.mean(values * values, axis=1, keepdims=True) + EPS)
    read_out[...] = values.astype(BF16)

    sent = pl.ds(OTHERS, 15)
    to_sp(kst.at[sent], kall.at[sent], ksend, krsem.at[0], OTHERS).wait_send()
    to_tp(qn.at[seven], qn.at[seven], qsend[0], qrsem.at[0], 1).wait_send()
    to_tp(qr.at[seven], qr.at[seven], qsend[1], qrsem.at[1], 1).wait_send()
    to_tp(pst.at[seven], pst.at[seven], psend, small.at[0], 1).wait_send()
    to_tp(aall.at[seven], aall.at[seven], asend, small.at[1], 1).wait_send()
    to_tp(asc.at[seven], arecv.at[seven], csend, small.at[2], 1).wait_send()
    to_tp(ktst.at[:, seven], ktst.at[:, seven], k2send, k2rsem.at[3], 1).wait_send()
    arrange(3)


def finish(stage, turned_stage, read_in, out_s, out_r, out_f, sem):
    pieces = 4
    for n in range(pieces):
        lanes = pl.ds(4096 // pieces * n, 4096 // pieces)
        pltpu.make_async_copy(stage.at[:, lanes], out_s.at[:, lanes], sem.at[0]).start()
    others = [
        pltpu.make_async_copy(turned_stage, out_r, sem.at[1]), pltpu.make_async_copy(read_in, out_f, sem.at[2])
    ]
    for c in others:
        c.start()
    pltpu.make_async_copy(stage, out_s, sem.at[0]).wait()
    for c in others:
        c.wait()


def solution(mesh):
    angles = trig_tables(128, 32, 64)

    def step(x, gain, w, rd, scal, look, payload, qn, qr):
        hbm = pl.BlockSpec(memory_space=pltpu.HBM)
        vmem = pl.BlockSpec(memory_space=pltpu.VMEM)
        dma = pltpu.SemaphoreType.DMA
        received = pl.pallas_call(
            kernel,
            out_shape=(
                jax.ShapeDtypeStruct((64, 4096), BF16),
                jax.ShapeDtypeStruct((8, 4096), BF16),
                jax.ShapeDtypeStruct((2, 128), BF16),
            ),
            in_specs=[hbm] * 10,
            out_specs=(vmem,) * 3,
            scratch_shapes=[
                pltpu.VMEM((16, 32, 2048), BF16),
                pltpu.VMEM((1, 2048), F32),
                pltpu.VMEM((2048, 640), BF16),
                pltpu.VMEM((64, 2048), BF16),
                pltpu.VMEM((1, 512), F32),
                pltpu.VMEM((1024, 128), BF16),
                pltpu.VMEM((1024, 128), BF16),
                pltpu.VMEM((168, 128), F32),
                pltpu.VMEM((16, 144, 128), BF16),
                pltpu.VMEM((16, 144, 128), BF16),
                pltpu.VMEM((8, 2, 128), BF16),
                pltpu.VMEM((8, 2, 64), BF16),
                pltpu.VMEM((8, 16, 128), BF16),
                pltpu.VMEM((8, 64, 256), BF16),
                pltpu.VMEM((512, 256), BF16),
                pltpu.VMEM((4, 8, 72, 128), BF16),
                pltpu.VMEM((4, 8, 72, 128), BF16),
                pltpu.VMEM((8, 2, 640), F32),
                pltpu.VMEM((8, 2, 640), F32),
                pltpu.VMEM((128, 512), F32),
                pltpu.VMEM((128, 2048), BF16),
                dma((2,)),
                dma((9,)),
                dma((4,)),
                dma((2,)),
                dma((3,)),
                dma((4,)),
            ],
            compiler_params=pltpu.CompilerParams(
                collective_id=0, has_side_effects=True, vmem_limit_bytes=48 * 1024 * 1024
            ),
        )(
            *(
                pltpu.with_memory_space_constraint(v, pltpu.HBM)
                for v in (
                    x, gain.reshape(1, 2048), w, rd.T, scal.reshape(1, 512), look.reshape(1024, 128),
                    payload.reshape(1024, 128), qn.reshape(2, 128), qr.reshape(2, 64),
                    jnp.asarray(angles),
                )
            )
        )
        stored, rotary, read = pl.pallas_call(
            finish,
            out_shape=(
                jax.ShapeDtypeStruct((64, 4096), BF16),
                jax.ShapeDtypeStruct((8, 4096), BF16),
                jax.ShapeDtypeStruct((2, 128), BF16),
            ),
            in_specs=[vmem] * 3,
            out_specs=(hbm,) * 3,
            scratch_shapes=[dma((3,))],
        )(*(pltpu.with_memory_space_constraint(v, pltpu.VMEM) for v in received))
        return stored.T[None], rotary.T[None], read[None]

    tp = "tp"
    both = ("sp", "tp")
    in_specs = (
        P(None, both, None), P(), P(), P(), P(), P(tp, None, None), P(tp, None, None),
        P("sp", tp, None), P("sp", tp, None),
    )
    out_specs = (P("sp", None, tp), P("sp", None, tp), P("sp", tp, None))
    return jax.shard_map(step, mesh=mesh, in_specs=in_specs, out_specs=out_specs, check_vma=False)
```
